32 devices in a mesh: sp: 16 (over z, y, x), tp: 2 (over core).
Axes of the slice: x: 2, y: 2, z: 4, core: 2. Of those that a mesh axis runs over, the one named last changes fastest.
Arguments:
- resid: bfloat16 [6144, 2048], P('sp', 'tp'), may hold values from -40 to 40
- query_one: bfloat16 [6144, 1024], P('sp', 'tp'), may hold values from -64 to 64
- key_one: bfloat16 [6144, 1024], P('sp', 'tp'), may hold values from -64 to 64
- query_two: bfloat16 [6144, 1024], P('sp', 'tp'), may hold values from -64 to 64
- key_two: bfloat16 [6144, 1024], P('sp', 'tp'), may hold values from -64 to 64
- values: bfloat16 [6144, 2048], P('sp', 'tp'), may hold values from -6 to 6
- mix_lambda: float32 [8], P('tp'), may hold values from 0.3 to 0.8
- segments: int32 [6144], P('sp'), may hold values from 0 to 7, never falling along the last dimension, each value on 1 to 1536 neighbouring positions
- head_gain: float32 [256], replicated, may hold values from 0.1 to 1.9
- out_weight: bfloat16 [2048, 2048], P(None, 'tp'), may hold values from -0.125 to 0.125
- mixer_gain: float32 [2048], P('tp'), may hold values from 0.1 to 1.9
- gate_weight: bfloat16 [2048, 6144], P('sp', 'tp'), may hold values from -0.125 to 0.125
- up_weight: bfloat16 [2048, 6144], P('sp', 'tp'), may hold values from -0.125 to 0.125
- down_weight: bfloat16 [6144, 2048], P('tp', 'sp'), may hold values from -0.078125 to 0.078125
Outputs:
- layer_out: bfloat16 [6144, 2048], P('sp', 'tp')
The draws below stay inside these ranges and needn't reach their ends.
Inputs may be any that keep to these rules, and one draw needn't show every extreme that they name: `segments`: numbers never fall along the sequence; each document has at most 1536 positions and one has exactly that many.
All inputs are finite; a program needn't handle non-finite values.
Results may differ from the reference program's by a relative error of at most 0.012.
Values may be sent and summed in bfloat16 or wider, within the bound.
A program may use at most 128 MiB of HBM per device.

```python
import math
import jax
import jax.numpy as jnp
import numpy as np
from jax import lax

D = 2048
HEADS = 8
HD = 128
VD = 256
FF = 6144
TOK_DEV = 384
REACH = 4
DOC_MOST = 1536
TOKENS = 6144
DOCS = 8
N_SP = 16
N_TP = 2


def draw_resid(key, part):
    base = jax.random.normal(jax.random.fold_in(key, 11), (TOKENS, D), jnp.float32)
    column = jnp.exp(1.6 * jnp.arange(D, dtype=jnp.float32) / D)
    result = base * column / 2.0
    return jnp.clip(result, -40.0, 40.0).astype(jnp.bfloat16)


def drawn_pair(key, which):
    pair_key = jax.random.fold_in(key, 100 + which)
    width = HEADS * HD
    query = 1.3 * jax.random.normal(jax.random.fold_in(pair_key, 1), (TOKENS, width), jnp.float32)
    keys = 1.3 * jax.random.normal(jax.random.fold_in(pair_key, 2), (TOKENS, width), jnp.float32)
    return (jnp.clip(query, -64.0, 64.0), jnp.clip(keys, -64.0, 64.0))


def draw_query_one(key, part):
    return drawn_pair(key, 1)[0].astype(jnp.bfloat16)


def draw_key_one(key, part):
    return drawn_pair(key, 1)[1].astype(jnp.bfloat16)


def draw_query_two(key, part):
    return drawn_pair(key, 2)[0].astype(jnp.bfloat16)


def draw_key_two(key, part):
    return drawn_pair(key, 2)[1].astype(jnp.bfloat16)


def level_of(own_key, dims, cuts, smallest, largest):
    factor_of = 1.0
    for dim, shards_of in cuts:
        draws = jax.random.uniform(jax.random.fold_in(jax.random.fold_in(own_key, 6), dim), (shards_of,), jnp.float32, smallest / len(cuts), largest / len(cuts))
        factor_of = factor_of * jnp.repeat(jnp.exp(draws), dims[dim] // shards_of).reshape((-1,) + (1,) * (len(dims) - 1 - dim))
    return factor_of


def length_profile(number_of, total, bound, lean):
    weights = [(1 << 20) // math.isqrt(grade ** lean) + 1 for grade in range(2, number_of + 1)]
    rest, counts = total - bound - (number_of - 1), [1] * (number_of - 1)
    while rest > 0:
        movable = [i for i in range(number_of - 1) if counts[i] < bound]
        pool, left = sum([weights[i] for i in movable]), rest
        for i in movable:
            addition = min(bound - counts[i], max(1, left * weights[i] // pool), rest)
            counts[i] = counts[i] + addition
            rest = rest - addition
    return np.array([bound] + counts)


def uneven_parts(rng, count, total, limit, slope):
    if count == 2:
        one = jax.random.randint(rng, (), max(1, total - limit), min(limit, total - 1) + 1)
        return jnp.stack([one, total - one])
    sizes = jnp.asarray(length_profile(count, total, limit, slope), jnp.int32)
    pairs = (count - 1) // 2
    giver, receiver = sizes[1:1 + 2 * pairs:2], sizes[2:2 + 2 * pairs:2]
    slack = jnp.minimum(giver - 1, limit - receiver)
    moved = jax.random.randint(jax.random.fold_in(rng, 1), (pairs,), 0, 1 << 20) % (slack + 1)
    sizes = sizes.at[1:1 + 2 * pairs:2].set(giver - moved).at[2:2 + 2 * pairs:2].set(receiver + moved)
    return sizes[jax.random.permutation(jax.random.fold_in(rng, 2), count)]


def normal_values(stream_key, dims, scale, reach, split=(), kind=jnp.bfloat16):
    values = jax.random.normal(stream_key, dims, jnp.float32) * scale
    if len(split) > 0:
        values = level_of(stream_key, dims, split, -0.22, 0.18) * values
    return jnp.clip(values, min=-reach, max=reach).astype(kind)


def setup_inputs(seed: int = 0) -> dict:
    arg_keys = jax.random.split(jax.random.key(seed), 15)
    resid = draw_resid(jax.random.fold_in(arg_keys[14], 71), 0)
    query_one = draw_query_one(jax.random.fold_in(arg_keys[14], 71), 0)
    key_one = draw_key_one(jax.random.fold_in(arg_keys[14], 71), 0)
    query_two = draw_query_two(jax.random.fold_in(arg_keys[14], 71), 0)
    key_two = draw_key_two(jax.random.fold_in(arg_keys[14], 71), 0)
    values = normal_values(arg_keys[5], (TOKENS, HEADS * VD), 1.0, 6.0, ((0, 16), (1, 2)))
    mix_lambda = jnp.clip(0.3 + 0.5 * jax.random.uniform(arg_keys[6], (HEADS,), jnp.float32) ** level_of(arg_keys[6], (HEADS,), ((0, 2),), -0.2, 0.2), 0.3, 0.8)
    segments = jnp.searchsorted(jnp.cumsum(uneven_parts(arg_keys[7], DOCS, TOKENS, DOC_MOST, 0)), jnp.arange(TOKENS), side="right").astype(jnp.int32)
    head_gain = jnp.clip(1.0 + 0.18 * jax.random.normal(arg_keys[8], (VD,), jnp.float32), 0.1, 1.9)
    out_weight = normal_values(arg_keys[9], (HEADS * VD, D), (HEADS * VD) ** -0.5, 0.125, ((1, 2),))
    mixer_gain = jnp.clip(1.0 + 0.18 * jax.random.normal(arg_keys[10], (D,), jnp.float32), 0.1, 1.9)
    gate_weight = normal_values(arg_keys[11], (D, FF), D ** -0.5, 0.125, ((0, 16), (1, 2)))
    up_weight = normal_values(arg_keys[12], (D, FF), D ** -0.5, 0.125, ((0, 16), (1, 2)))
    down_weight = normal_values(arg_keys[13], (FF, D), FF ** -0.5, 0.078125, ((0, 2), (1, 16)))
    return {"resid": resid, "query_one": query_one, "key_one": key_one, "query_two": query_two, "key_two": key_two, "values": values, "mix_lambda": mix_lambda, "segments": segments, "head_gain": head_gain, "out_weight": out_weight, "mixer_gain": mixer_gain, "gate_weight": gate_weight, "up_weight": up_weight, "down_weight": down_weight}


def reference(resid, query_one, key_one, query_two, key_two, values, mix_lambda, segments, head_gain, out_weight, mixer_gain, gate_weight, up_weight, down_weight):
    rows = TOK_DEV
    span = REACH * TOK_DEV

    def padded(array):
        return jnp.concatenate([jnp.zeros((span,) + array.shape[1:], array.dtype), array], 0)
    key_first = padded(key_one)
    key_second = padded(key_two)
    value_pad = padded(values)
    seg_pad = jnp.concatenate([jnp.full((span,), -1, jnp.int32), segments.astype(jnp.int32)], 0)

    def block(index):
        start = (index * rows).astype(jnp.int32)
        width = span + rows
        q_first = lax.dynamic_slice_in_dim(query_one, start, rows, 0).reshape(rows, HEADS, HD).astype(jnp.float32)
        q_second = lax.dynamic_slice_in_dim(query_two, start, rows, 0).reshape(rows, HEADS, HD).astype(jnp.float32)
        k_first = lax.dynamic_slice_in_dim(key_first, start, width, 0).reshape(width, HEADS, HD).astype(jnp.float32)
        k_second = lax.dynamic_slice_in_dim(key_second, start, width, 0).reshape(width, HEADS, HD).astype(jnp.float32)
        vals = lax.dynamic_slice_in_dim(value_pad, start, width, 0).reshape(width, HEADS, VD).astype(jnp.float32)
        seg_query = lax.dynamic_slice_in_dim(segments.astype(jnp.int32), start, rows, 0)
        seg_key = lax.dynamic_slice_in_dim(seg_pad, start, width, 0)
        q_pos = start + jnp.arange(rows, dtype=jnp.int32)
        k_pos = start - span + jnp.arange(width, dtype=jnp.int32)
        allowed = (seg_key[None, :] == seg_query[:, None]) & (k_pos[None, :] <= q_pos[:, None]) & (k_pos[None, :] >= 0)

        def weights(query, keys):
            score = jnp.einsum('qhd,khd->hqk', query, keys) * HD ** (-0.5)
            score = jnp.where(allowed[None], score, -jnp.inf)
            score = score - lax.optimization_barrier(jnp.max(score, axis=-1, keepdims=True))
            expo = jnp.exp(score)
            return (expo / lax.optimization_barrier(jnp.sum(expo, axis=-1, keepdims=True))).astype(jnp.bfloat16)
        probs_first = weights(q_first, k_first).astype(jnp.float32)
        probs_second = weights(q_second, k_second).astype(jnp.float32)
        out_first = jnp.einsum('hqk,khe->qhe', probs_first, vals)
        out_second = jnp.einsum('hqk,khe->qhe', probs_second, vals)
        head_out = out_first - mix_lambda[None, :, None] * out_second
        meansq = lax.optimization_barrier(jnp.mean(head_out * head_out, axis=-1, keepdims=True))
        normal = head_out * lax.rsqrt(meansq + 1e-05) * head_gain
        return normal.reshape(rows, HEADS * VD).astype(jnp.bfloat16)
    attn_rows = lax.map(block, jnp.arange(N_SP, dtype=jnp.int32)).reshape(TOKENS, HEADS * VD)
    mid = (resid.astype(jnp.float32) + jnp.dot(attn_rows, out_weight, preferred_element_type=jnp.float32)).astype(jnp.bfloat16)
    midf = mid.astype(jnp.float32)
    meansq = lax.optimization_barrier(jnp.mean(midf * midf, axis=-1, keepdims=True))
    normed = (midf * lax.rsqrt(meansq + 1e-06) * mixer_gain).astype(jnp.bfloat16)
    gate = jnp.dot(normed, gate_weight, preferred_element_type=jnp.float32)
    up = jnp.dot(normed, up_weight, preferred_element_type=jnp.float32)
    hidden = (jax.nn.silu(gate) * up).astype(jnp.bfloat16)
    blocks = FF // N_TP
    hidden_blocks = hidden.reshape(TOKENS, N_TP, blocks).transpose(1, 0, 2)
    down_blocks = down_weight.reshape(N_TP, blocks, D)

    def add_block(total, pair):
        part = jnp.dot(pair[0], pair[1], preferred_element_type=jnp.float32).astype(jnp.bfloat16)
        part = lax.optimization_barrier(part)
        return (total + part.astype(jnp.float32), None)
    summed, unused = lax.scan(add_block, jnp.zeros((TOKENS, D), jnp.float32), (hidden_blocks, down_blocks))
    return (midf + summed).astype(jnp.bfloat16)
```

```python
import functools

import jax
import jax.numpy as jnp
from jax import lax
from jax.experimental import pallas as pl
from jax.experimental.pallas import tpu as pltpu
from jax.sharding import PartitionSpec as P

HD = 128
VD = 256
REACH = 4
SHARE = 2


def shifted(value, axis, by):
    length = lax.axis_size(axis)
    pairs = [(i, i + by) for i in range(length) if 0 <= i + by < length]
    return lax.ppermute(value, axis, pairs)


def groups(length):
    share = SHARE if length % SHARE == 0 else 1
    plane = [[i * share + j for j in range(share)] for i in range(length // share)]
    across = [[i * share + j for i in range(length // share)] for j in range(share)]
    return plane, across


def spread(blocks):
    length = lax.axis_size("sp")
    share = blocks.shape[0]
    if share == 1:
        return blocks
    mine = lax.rem(lax.axis_index("sp"), share)
    own = lax.dynamic_index_in_dim(blocks, mine, 0, keepdims=True)
    result = lax.dynamic_update_slice_in_dim(jnp.zeros_like(blocks), own, mine, 0)
    for by in range(1, share):
        pairs = [(i, i - i % share + (i + by) % share) for i in range(length)]
        sent = lax.dynamic_index_in_dim(blocks, lax.rem(mine + by, share), 0, keepdims=True)
        came = lax.ppermute(sent, "sp", pairs)
        result = lax.dynamic_update_slice_in_dim(result, came, lax.rem(mine + share - by, share), 0)
    return result


def gathered(gate_weight, up_weight, down_weight):
    plane, across = groups(lax.axis_size("sp"))
    share = len(plane[0])
    depth, units = gate_weight.shape
    part = units // share
    both = [gate_weight.reshape(depth, share, part), up_weight.reshape(depth, share, part)]
    both = jnp.concatenate(both, 2).transpose(1, 0, 2)
    both = spread(both).reshape(share * depth, 2 * part)
    down = spread(down_weight.reshape(share, part, depth))
    down = down.transpose(1, 0, 2).reshape(part, share * depth)
    both = lax.all_gather(both, "sp", axis=0, tiled=True, axis_index_groups=across)
    down = lax.all_gather(down, "sp", axis=1, tiled=True, axis_index_groups=across)
    return both, down


def swapped(value, axis, members):
    return lax.ppermute(value, axis, [(i, i ^ 1) for i in range(members)])


def whole_channels(value):
    members = lax.axis_size("tp")
    if members != 2:
        return lax.all_gather(value, "tp", axis=1, tiled=True)
    other = swapped(value, "tp", members)
    mine = lax.axis_index("tp") * value.shape[1]
    result = jnp.zeros((value.shape[0], 2 * value.shape[1]), value.dtype)
    result = lax.dynamic_update_slice_in_dim(result, value, mine, 1)
    return lax.dynamic_update_slice_in_dim(result, other, value.shape[1] - mine, 1)


def own_channels(terms):
    members = lax.axis_size("tp")
    if members != 2:
        return lax.psum_scatter(terms, "tp", scatter_dimension=1, tiled=True).astype(jnp.float32)
    width = terms.shape[1] // 2
    mine = lax.axis_index("tp") * width
    other = swapped(lax.dynamic_slice_in_dim(terms, width - mine, width, 1), "tp", members)
    own = lax.dynamic_slice_in_dim(terms, mine, width, 1)
    return own.astype(jnp.float32) + other.astype(jnp.float32)


def body(
    resid,
    query_one,
    key_one,
    query_two,
    key_two,
    values,
    mix_lambda,
    segments,
    head_gain,
    out_weight,
    mixer_gain,
    gate_weight,
    up_weight,
    down_weight,
):
    rows = query_one.shape[0]
    heads = mix_lambda.shape[0]
    position = lax.axis_index("sp")
    both_all, down_all = gathered(gate_weight, up_weight, down_weight)
    carried = (key_one, key_two, values, segments)
    earlier = [carried]
    for step in range(REACH):
        carried = shifted((carried[0], carried[1], carried[2], carried[3]), "sp", 1)
        earlier.insert(0, carried)
    width = (REACH + 1) * rows
    k_first = jnp.concatenate([piece[0] for piece in earlier], 0).reshape(width, heads, HD)
    k_second = jnp.concatenate([piece[1] for piece in earlier], 0).reshape(width, heads, HD)
    vals = jnp.concatenate([piece[2] for piece in earlier], 0).reshape(width, heads, VD)
    seg_key = jnp.concatenate([piece[3] for piece in earlier], 0)
    q_pos = position * rows + jnp.arange(rows, dtype=jnp.int32)
    k_pos = (position - REACH) * rows + jnp.arange(width, dtype=jnp.int32)
    allowed = (
        (seg_key[None, :] == segments[:, None])
        & (k_pos[None, :] <= q_pos[:, None])
        & (k_pos[None, :] >= 0)
    )

    def weights(query, keys):
        score = jnp.einsum(
            "qhd,khd->hqk", query.reshape(rows, heads, HD), keys, preferred_element_type=jnp.float32
        ) * HD ** (-0.5)
        score = jnp.where(allowed[None], score, -jnp.inf)
        score = score - jnp.max(score, axis=-1, keepdims=True)
        expo = jnp.exp(score)
        return (expo / jnp.sum(expo, axis=-1, keepdims=True)).astype(jnp.bfloat16)

    out_first = jnp.einsum(
        "hqk,khe->qhe", weights(query_one, k_first), vals, preferred_element_type=jnp.float32
    )
    out_second = jnp.einsum(
        "hqk,khe->qhe", weights(query_two, k_second), vals, preferred_element_type=jnp.float32
    )
    head_out = out_first - mix_lambda[None, :, None] * out_second
    meansq = jnp.mean(head_out * head_out, axis=-1, keepdims=True)
    attn_rows = (
        (head_out * lax.rsqrt(meansq + 1e-05) * head_gain)
        .reshape(rows, heads * VD)
        .astype(jnp.bfloat16)
    )
    projected = jnp.dot(
        whole_channels(attn_rows),
        out_weight,
        preferred_element_type=jnp.float32,
    )
    mid = (resid.astype(jnp.float32) + projected).astype(jnp.bfloat16)
    midf = mid.astype(jnp.float32)
    squares = lax.psum(jnp.sum(midf * midf, axis=1), "tp")
    channels = mid.shape[1] * lax.axis_size("tp")
    normed = (midf * lax.rsqrt(squares / channels + 1e-06)[:, None] * mixer_gain).astype(
        jnp.bfloat16
    )
    members = lax.axis_size("sp")
    paired = len(groups(members)[0][0]) == 2
    if paired:
        normed = jnp.concatenate([normed, swapped(normed, "sp", members)], 0)
    whole_rows = whole_channels(normed)
    whole_rows, both_all, down_all = lax.optimization_barrier((whole_rows, both_all, down_all))
    part = both_all.shape[1] // 2
    gate = jnp.dot(whole_rows, both_all[:, :part], preferred_element_type=jnp.float32)
    up = jnp.dot(whole_rows, both_all[:, part:], preferred_element_type=jnp.float32)
    hidden = (jax.nn.silu(gate) * up).astype(jnp.bfloat16)
    terms = jnp.dot(hidden, down_all, preferred_element_type=jnp.float32)
    summed = own_channels(terms.astype(jnp.bfloat16))
    if paired:
        came = swapped(summed[rows:].astype(jnp.bfloat16), "sp", members)
        summed = summed[:rows] + came.astype(jnp.float32)
    return (midf + summed).astype(jnp.bfloat16)


def rdma(src, dst, send, recv, device):
    return pltpu.make_async_remote_copy(
        src_ref=src, dst_ref=dst, send_sem=send, recv_sem=recv,
        device_id=device, device_id_type=pl.DeviceIdType.MESH,
    )


def layer_kernel(
    plane, lines, sub,
    resid, q_one, k_one, q_two, k_two, vals, lam, seg, head_gain, out_w, mix_gain, gate, up, down,
    out,
    qb, kb, vb, sb, ao, ar, oww, res, mid, mg, xa, ga, ua, da, hid, pown, psend, precv, csend, crecv,
    s_qkv, r_qkv, s_halo, r_halo, s_w1, s_w2, r_w, s_ao, r_ao, s_pair, r_pair,
    s_ag, r_ag, s_xd, r_xd, s_pp, r_pp, s_ch, r_ch, s_loc,
):
    sp, tp = lax.axis_index("sp"), lax.axis_index("tp")
    z, p = lax.div(sp, plane), lax.rem(sp, plane)
    rows, half = resid.shape
    heads = plane
    depth = gate.shape[0]
    units = gate.shape[1] // lines
    own_rows = plane * rows
    px, py = lax.rem(p, 2), lax.div(p, 2)

    def peer(k):
        a, b = k % 2, k // 2
        return (py + b - 2 * py * b) * 2 + px + a - 2 * px * a

    def line_peer(d):
        return lax.rem(z + d, lines)

    partner = (sp, 1 - tp)
    in_plane = [peer(k) for k in range(1, plane)]

    barrier = pltpu.get_barrier_semaphore()
    for q in in_plane:
        pl.semaphore_signal(barrier, inc=1, device_id=(z * plane + q, tp), device_id_type=pl.DeviceIdType.MESH)
    for d in range(1, lines):
        pl.semaphore_signal(barrier, inc=1, device_id=(line_peer(d) * plane + p, tp), device_id_type=pl.DeviceIdType.MESH)
    pl.semaphore_signal(barrier, inc=1, device_id=partner, device_id_type=pl.DeviceIdType.MESH)
    pl.semaphore_wait(barrier, plane - 1 + lines - 1 + 1)

    sources = (k_one, k_two, vals, q_one, q_two)

    def mul(i, n):
        return pl.multiple_of(i * n, n)

    def qkv_src(a, head):
        wide = VD if a == 2 else HD
        return sources[a].at[:, pl.ds(mul(head, wide), wide)]

    def kv_dst(a, block):
        at = pl.ds(mul(block, rows), rows)
        if a == 2:
            return vb.at[at, :]
        return kb.at[a, at, :]

    def qkv_dst(a, block):
        if a == 5:
            return sb.at[plane + block]
        if a < 3:
            return kv_dst(a, plane + block)
        return qb.at[a - 3, pl.ds(mul(block, rows), rows), :]

    def qkv_copy(k, a):
        q = in_plane[k]
        src = seg if a == 5 else qkv_src(a, q)
        return rdma(src, qkv_dst(a, p), s_qkv.at[k, a], r_qkv.at[p, a], (z * plane + q, tp))

    def halo_copy(block, a, own):
        if a == 3:
            src = seg if own else sb.at[plane + block]
            dst = sb.at[block]
        else:
            src = qkv_src(a, p) if own else kv_dst(a, plane + block)
            dst = kv_dst(a, block)
        return rdma(src, dst, s_halo.at[block, a], r_halo.at[block, a], (sp + plane, tp))

    def weight_dst(s, a):
        if a == 0:
            return ga.at[pl.ds(mul(s, depth), depth), :]
        if a == 1:
            return ua.at[pl.ds(mul(s, depth), depth), :]
        return da.at[:, pl.ds(mul(s, depth), depth)]

    def weight_src(line, a):
        at = pl.ds(mul(line, units), units)
        if a == 0:
            return gate.at[:, at]
        if a == 1:
            return up.at[:, at]
        return down.at[at, :]

    def w1_copy(d, a):
        zz = line_peer(d)
        return rdma(weight_src(zz, a), weight_dst(sp, a), s_w1.at[d - 1, a], r_w.at[sp, a], (zz * plane + p, tp))

    def w2_copy(k, d, a):
        s = line_peer(d) * plane + p
        src = weight_src(z, a) if d == 0 else weight_dst(s, a)
        return rdma(src, weight_dst(s, a), s_w2.at[k, d, a], r_w.at[s, a], (z * plane + in_plane[k], tp))

    def arrived(dst, sem):
        rdma(dst, dst, s_pair.at[0], sem, partner).wait_recv()

    def local(src, dst, i):
        return pltpu.make_async_copy(src, dst, s_loc.at[i])

    for a in (0, 1, 2, 5):
        for k in range(plane - 1):
            qkv_copy(k, a).start()
    for k in range(plane - 1):
        for a in (3, 4):
            qkv_copy(k, a).start()

    @pl.when(z < lines - 1)
    def _():
        for a in range(4):
            halo_copy(p, a, True).start()

    for d in range(1, lines):
        w1_copy(d, 0).start()

    locals_ = [local(qkv_src(a, p), qkv_dst(a, p), a) for a in range(5)]
    locals_.append(local(out_w, oww, 5))
    locals_.append(local(resid, res, 6))
    for a in range(3):
        locals_.append(local(weight_src(z, a), weight_dst(sp, a), 7 + a))
    for c in locals_:
        c.start()
    sb[plane + p] = seg[...]
    mg[tp] = mix_gain[...]
    rdma(mix_gain, mg.at[tp], s_pair.at[0], r_pair.at[0], partner).start()

    for a in range(3):
        for k in range(plane - 1):
            w2_copy(k, 0, a).start()

    @pl.when(z == 0)
    def _():
        vb[: plane * rows, :] = jnp.zeros((plane * rows, VD), vb.dtype)
        kb[:, : plane * rows, :] = jnp.zeros((2, plane * rows, HD), kb.dtype)
        for b in range(plane):
            sb[b] = jnp.full(sb.shape[1:], -1, sb.dtype)

    for k in range(plane - 1):
        q = in_plane[k]
        for a in (0, 1, 2, 5):
            arrived(qkv_dst(a, q), r_qkv.at[q, a])

        @pl.when(z < lines - 1)
        def _():
            for a in range(4):
                halo_copy(q, a, False).start()

    for d in range(1, lines):
        for a in (1, 2):
            w1_copy(d, a).start()
    for k in range(plane - 1):
        q = in_plane[k]
        for a in (3, 4):
            arrived(qkv_dst(a, q), r_qkv.at[q, a])
    for c in locals_[:5]:
        c.wait()

    def forward_weights(a):
        for d in range(1, lines):
            s = line_peer(d) * plane + p
            arrived(weight_dst(s, a), r_w.at[s, a])
            for k in range(plane - 1):
                w2_copy(k, d, a).start()

    forward_weights(0)

    scale = HD ** (-0.5) * 1.4426950408889634
    window = (REACH + 1) * rows

    def ao_remote(j):
        at = pl.ds(mul(tp * heads + p, VD), VD)
        return rdma(ao.at[j], ar.at[:, at], s_ao.at[j], r_ao.at[p], (z * plane + j, tp))

    def ao_local(j):
        at = pl.ds(mul(tp * heads + p, VD), VD)
        return local(ao.at[j], ar.at[:, at], 10)

    coef = lam[p]

    def query_block(i, carry):
        j = plane - 1 - i

        @pl.when(z > 0)
        def _():
            for a in range(3):
                arrived(kv_dst(a, j), r_halo.at[j, a])
            arrived(sb.at[j], r_halo.at[j, 3])

        at = pl.ds(mul(j, rows), window)
        key_seg = jnp.concatenate([sb[j + n] for n in range(REACH + 1)], axis=1).astype(jnp.float32)
        own_seg = jnp.broadcast_to(sb[plane + j].astype(jnp.float32), (128, rows))
        seg_col = jnp.transpose(own_seg)[:, :1]
        for u in range(rows // sub):
            col = lax.broadcasted_iota(jnp.int32, (sub, window), 1)
            row = lax.broadcasted_iota(jnp.int32, (sub, window), 0) + (REACH * rows + u * sub)
            ok = (key_seg == seg_col[u * sub : (u + 1) * sub]) & (col <= row)
            outs = []
            for m in range(2):
                q = qb[m, pl.ds(pl.multiple_of(j * rows + u * sub, sub), sub), :]
                s = lax.dot_general(
                    q, kb[m, at, :], (((1,), (1,)), ((), ())), preferred_element_type=jnp.float32
                )
                s = jnp.where(ok, s, -1e30)
                top = jnp.max(s, axis=1, keepdims=True)
                e = jnp.exp2((s - top) * scale)
                total = jnp.sum(e, axis=1, keepdims=True)
                o = jnp.dot(e.astype(jnp.bfloat16), vb[at, :], preferred_element_type=jnp.float32)
                outs.append(o / total)
            h = outs[0] - coef * outs[1]
            ms = jnp.mean(h * h, axis=1, keepdims=True)
            h = h * lax.rsqrt(ms + 1e-05) * head_gain[...]
            ao[j, pl.ds(u * sub, sub), :] = h.astype(ao.dtype)

        @pl.when(j != p)
        def _():
            ao_remote(j).start()

        @pl.when(j == p)
        def _():
            ao_local(j).start()

        return carry

    lax.fori_loop(0, plane, query_block, 0)

    ao_local(p).wait()
    for q in in_plane:
        at = pl.ds(mul(tp * heads + q, VD), VD)
        arrived(ar.at[:, at], r_ao.at[q])
    mine = pl.ds(mul(tp, half), half)
    theirs = pl.ds(mul(1 - tp, half), half)
    swap = rdma(ar.at[:, mine], ar.at[:, mine], s_pair.at[1], r_pair.at[1], partner)
    swap.start()
    for c in locals_[5:7]:
        c.wait()
    acc = jnp.dot(ar[:, mine], oww[mine, :], preferred_element_type=jnp.float32)
    arrived(ar.at[:, theirs], r_pair.at[1])
    acc = acc + jnp.dot(ar[:, theirs], oww[theirs, :], preferred_element_type=jnp.float32)
    mid[tp] = (res[...].astype(jnp.float32) + acc).astype(mid.dtype)
    swap_mid = rdma(mid.at[tp], mid.at[tp], s_pair.at[2], r_pair.at[2], partner)
    swap_mid.start()
    arrived(mid.at[1 - tp], r_pair.at[2])
    arrived(mg.at[1 - tp], r_pair.at[0])
    m0, m1 = mid[0].astype(jnp.float32), mid[1].astype(jnp.float32)
    squares = jnp.sum(m0 * m0, axis=1, keepdims=True) + jnp.sum(m1 * m1, axis=1, keepdims=True)
    inv = lax.rsqrt(squares / (2 * half) + 1e-06)
    xa[z, 0] = (m0 * inv * mg[0]).astype(xa.dtype)
    xa[z, 1] = (m1 * inv * mg[1]).astype(xa.dtype)

    def ag_copy(b, to):
        return rdma(xa.at[b, tp], xa.at[b, tp], s_ag.at[b, to], r_ag.at[b], (sp + plane * (2 * to - 1), tp))

    def xd_copy(b):
        return rdma(xa.at[b, tp], xa.at[b, tp], s_xd.at[b], r_xd.at[b], partner)

    @pl.when(z < lines - 1)
    def _():
        ag_copy(z, 1).start()

    @pl.when(z > 0)
    def _():
        ag_copy(z, 0).start()

    def gather_step(d):
        below, above = z - d, z + d

        @pl.when(below >= 0)
        def _():
            arrived(xa.at[below, tp], r_ag.at[below])

            @pl.when(z < lines - 1)
            def _():
                ag_copy(below, 1).start()

            xd_copy(below).start()

        @pl.when(above < lines)
        def _():
            arrived(xa.at[above, tp], r_ag.at[above])

            @pl.when(z > 0)
            def _():
                ag_copy(above, 0).start()

            xd_copy(above).start()

    forward_weights(1)
    gather_step(1)
    forward_weights(2)
    for d in range(2, lines):
        gather_step(d)

    for c in locals_[7:]:
        c.wait()
    for k in range(plane - 1):
        for d in range(lines):
            s = line_peer(d) * plane + in_plane[k]
            for a in range(3):
                arrived(weight_dst(s, a), r_w.at[s, a])

    low = 2 * z < lines

    def order(i):
        down_first = jnp.where(i < lines - 1 - z, lines - 1 - i, i - (lines - 1 - z))
        up_first = jnp.where(i < z, i, lines - 1 - (i - z))
        b = jnp.where(low, down_first, up_first)
        return jnp.where(i == lines - 1, z, b)

    tile = units // 3

    def mixer(i):
        b = order(i)

        @pl.when(b != z)
        def _():
            arrived(xa.at[b, 1 - tp], r_xd.at[b])

        def hidden_tile(u, carry):
            at = pl.ds(mul(u, tile), tile)
            g = jnp.dot(xa[b, 0], ga[:half, at], preferred_element_type=jnp.float32)
            g = g + jnp.dot(xa[b, 1], ga[half:, at], preferred_element_type=jnp.float32)
            v = jnp.dot(xa[b, 0], ua[:half, at], preferred_element_type=jnp.float32)
            v = v + jnp.dot(xa[b, 1], ua[half:, at], preferred_element_type=jnp.float32)
            hid[:, at] = (g / (1.0 + jnp.exp(-g)) * v).astype(hid.dtype)
            return carry

        lax.fori_loop(0, units // tile, hidden_tile, 0)
        wide = half // 2

        def down_tile(c, carry):
            theirs_at = pl.ds(pl.multiple_of((1 - tp) * half + c * wide, wide), wide)
            own_at = pl.ds(pl.multiple_of(tp * half + c * wide, wide), wide)
            at = pl.ds(mul(c, wide), wide)
            o = jnp.dot(hid[...], da[:, theirs_at], preferred_element_type=jnp.float32)
            psend[b, :, at] = o.astype(psend.dtype)
            o = jnp.dot(hid[...], da[:, own_at], preferred_element_type=jnp.float32)
            pown[b, :, at] = o
            return carry

        lax.fori_loop(0, half // wide, down_tile, 0)
        rdma(psend.at[b], precv.at[b], s_pp.at[b], r_pp.at[b], partner).start()

    def chain_copy(b, to):
        near = jnp.where(b == z + 1, lines, b) if to == 1 else b
        return rdma(csend.at[b], crecv.at[near], s_ch.at[b], r_ch.at[near], (sp + plane * (2 * to - 1), tp))

    def chain(i):
        b = order(i)
        arrived(precv.at[b], r_pp.at[b])
        incoming = ((b < z) & (z < lines - 1)) | ((b > z) & (z > 0))

        @pl.when(incoming)
        def _():
            arrived(crecv.at[b], r_ch.at[b])
            csend[b] = (pown[b] + precv[b].astype(jnp.float32) + crecv[b].astype(jnp.float32)).astype(csend.dtype)

        @pl.when(jnp.logical_not(incoming))
        def _():
            csend[b] = (pown[b] + precv[b].astype(jnp.float32)).astype(csend.dtype)

        @pl.when(b > z)
        def _():
            chain_copy(b, 1).start()

        @pl.when(b < z)
        def _():
            chain_copy(b, 0).start()

    def mixer_step(i, carry):
        mixer(i)

        @pl.when(i > 0)
        def _():
            chain(i - 1)

        return carry

    lax.fori_loop(0, lines, mixer_step, 0)
    arrived(precv.at[z], r_pp.at[z])
    pown[z] = pown[z] + precv[z].astype(jnp.float32) + mid[tp].astype(jnp.float32)

    @pl.when(z < lines - 1)
    def _():
        arrived(crecv.at[z], r_ch.at[z])
        pown[z] = pown[z] + crecv[z].astype(jnp.float32)

    @pl.when(z > 0)
    def _():
        arrived(crecv.at[lines], r_ch.at[lines])
        pown[z] = pown[z] + crecv[lines].astype(jnp.float32)

    out[...] = pown[z].astype(out.dtype)

    for k in range(plane - 1):
        for a in range(6):
            qkv_copy(k, a).wait_send()
        for d in range(lines):
            for a in range(3):
                w2_copy(k, d, a).wait_send()
    for d in range(1, lines):
        for a in range(3):
            w1_copy(d, a).wait_send()

    @pl.when(z < lines - 1)
    def _():
        for a in range(4):
            halo_copy(p, a, True).wait_send()
            for q in in_plane:
                halo_copy(q, a, False).wait_send()

    for q in in_plane:
        ao_remote(q).wait_send()
    rdma(mix_gain, mg.at[tp], s_pair.at[0], r_pair.at[0], partner).wait_send()
    swap.wait_send()
    swap_mid.wait_send()
    for b in range(lines):
        rdma(psend.at[b], precv.at[b], s_pp.at[b], r_pp.at[b], partner).wait_send()

        @pl.when(b != z)
        def _():
            xd_copy(b).wait_send()

        @pl.when((b <= z) & (z < lines - 1))
        def _():
            ag_copy(b, 1).wait_send()

        @pl.when((b >= z) & (z > 0))
        def _():
            ag_copy(b, 0).wait_send()

        @pl.when(b > z)
        def _():
            chain_copy(b, 1).wait_send()

        @pl.when(b < z)
        def _():
            chain_copy(b, 0).wait_send()


def fast_body(resid, query_one, key_one, query_two, key_two, values, mix_lambda, segments, head_gain,
              out_weight, mixer_gain, gate_weight, up_weight, down_weight):
    plane = mix_lambda.shape[0]
    lines = lax.axis_size("sp") // plane
    rows, half = resid.shape
    depth, units = gate_weight.shape[0], gate_weight.shape[1] // lines
    full = depth * plane * lines
    bf, f32 = jnp.bfloat16, jnp.float32
    sub = rows // 3
    dma = pltpu.SemaphoreType.DMA
    anywhere = pl.BlockSpec(memory_space=pl.ANY)
    vmem = pl.BlockSpec(memory_space=pltpu.VMEM)
    smem = pl.BlockSpec(memory_space=pltpu.SMEM)
    flops = 6 * rows * plane * full * units + 2 * rows * full * half + 24 * rows * plane * rows * 5 * VD
    return pl.pallas_call(
        functools.partial(layer_kernel, plane, lines, sub),
        out_shape=jax.ShapeDtypeStruct((rows, half), bf),
        in_specs=[anywhere] * 6 + [smem, vmem, vmem, anywhere, vmem, anywhere, anywhere, anywhere],
        out_specs=vmem,
        scratch_shapes=[
            pltpu.VMEM((2, plane * rows, HD), bf),
            pltpu.VMEM((2, 2 * plane * rows, HD), bf),
            pltpu.VMEM((2 * plane * rows, VD), bf),
            pltpu.VMEM((2 * plane, 1, rows), jnp.int32),
            pltpu.VMEM((plane, rows, VD), bf),
            pltpu.VMEM((rows, full), bf),
            pltpu.VMEM((full, half), bf),
            pltpu.VMEM((rows, half), bf),
            pltpu.VMEM((2, rows, half), bf),
            pltpu.VMEM((2, 1, half), f32),
            pltpu.VMEM((lines, 2, rows, half), bf),
            pltpu.VMEM((full, units), bf),
            pltpu.VMEM((full, units), bf),
            pltpu.VMEM((units, full), bf),
            pltpu.VMEM((rows, units), bf),
            pltpu.VMEM((lines, rows, half), f32),
            pltpu.VMEM((lines, rows, half), bf),
            pltpu.VMEM((lines, rows, half), bf),
            pltpu.VMEM((lines, rows, half), bf),
            pltpu.VMEM((lines + 1, rows, half), bf),
            dma((plane - 1, 6)), dma((plane, 6)),
            dma((plane, 4)), dma((plane, 4)),
            dma((lines - 1, 3)), dma((plane - 1, lines, 3)), dma((plane * lines, 3)),
            dma((plane,)), dma((plane,)),
            dma((3,)), dma((3,)),
            dma((lines, 2)), dma((lines,)),
            dma((lines,)), dma((lines,)),
            dma((lines,)), dma((lines,)),
            dma((lines,)), dma((lines + 1,)),
            dma((11,)),
        ],
        compiler_params=pltpu.CompilerParams(
            collective_id=0, has_side_effects=True, vmem_limit_bytes=60 * 1024 * 1024
        ),
        cost_estimate=pl.CostEstimate(flops=flops, bytes_accessed=2 * full * units, transcendentals=0),
        name="layer",
    )(resid, query_one, key_one, query_two, key_two, values, mix_lambda, segments.reshape(1, rows),
      head_gain.reshape(1, VD), out_weight, mixer_gain.reshape(1, half), gate_weight, up_weight, down_weight)


def fits(mesh):
    sp, tp = mesh.shape["sp"], mesh.shape["tp"]
    return tp == 2 and sp % (REACH * 2) == 0


def choose(mesh):
    def step(*args):
        heads = args[6].shape[0]
        if fits(mesh) and heads == REACH:
            return fast_body(*args)
        return body(*args)

    return step


def solution(mesh):
    in_specs = (
        P("sp", "tp"),
        P("sp", "tp"),
        P("sp", "tp"),
        P("sp", "tp"),
        P("sp", "tp"),
        P("sp", "tp"),
        P("tp"),
        P("sp"),
        P(),
        P(None, "tp"),
        P("tp"),
        P("sp", "tp"),
        P("sp", "tp"),
        P("tp", "sp"),
    )
    out_specs = P("sp", "tp")
    return jax.shard_map(choose(mesh), mesh=mesh, in_specs=in_specs, out_specs=out_specs, check_vma=False)
```

```python
import functools

import jax
import jax.numpy as jnp
from jax import lax
from jax.experimental import pallas as pl
from jax.experimental.pallas import tpu as pltpu
from jax.sharding import PartitionSpec as P

HD = 128
VD = 256
REACH = 4
SHARE = 2


def shifted(value, axis, by):
    length = lax.axis_size(axis)
    pairs = [(i, i + by) for i in range(length) if 0 <= i + by < length]
    return lax.ppermute(value, axis, pairs)


def groups(length):
    share = SHARE if length % SHARE == 0 else 1
    plane = [[i * share + j for j in range(share)] for i in range(length // share)]
    across = [[i * share + j for i in range(length // share)] for j in range(share)]
    return plane, across


def spread(blocks):
    length = lax.axis_size("sp")
    share = blocks.shape[0]
    if share == 1:
        return blocks
    mine = lax.rem(lax.axis_index("sp"), share)
    own = lax.dynamic_index_in_dim(blocks, mine, 0, keepdims=True)
    result = lax.dynamic_update_slice_in_dim(jnp.zeros_like(blocks), own, mine, 0)
    for by in range(1, share):
        pairs = [(i, i - i % share + (i + by) % share) for i in range(length)]
        sent = lax.dynamic_index_in_dim(blocks, lax.rem(mine + by, share), 0, keepdims=True)
        came = lax.ppermute(sent, "sp", pairs)
        result = lax.dynamic_update_slice_in_dim(result, came, lax.rem(mine + share - by, share), 0)
    return result


def gathered(gate_weight, up_weight, down_weight):
    plane, across = groups(lax.axis_size("sp"))
    share = len(plane[0])
    depth, units = gate_weight.shape
    part = units // share
    both = [gate_weight.reshape(depth, share, part), up_weight.reshape(depth, share, part)]
    both = jnp.concatenate(both, 2).transpose(1, 0, 2)
    both = spread(both).reshape(share * depth, 2 * part)
    down = spread(down_weight.reshape(share, part, depth))
    down = down.transpose(1, 0, 2).reshape(part, share * depth)
    both = lax.all_gather(both, "sp", axis=0, tiled=True, axis_index_groups=across)
    down = lax.all_gather(down, "sp", axis=1, tiled=True, axis_index_groups=across)
    return both, down


def swapped(value, axis, members):
    return lax.ppermute(value, axis, [(i, i ^ 1) for i in range(members)])


def whole_channels(value):
    members = lax.axis_size("tp")
    if members != 2:
        return lax.all_gather(value, "tp", axis=1, tiled=True)
    other = swapped(value, "tp", members)
    mine = lax.axis_index("tp") * value.shape[1]
    result = jnp.zeros((value.shape[0], 2 * value.shape[1]), value.dtype)
    result = lax.dynamic_update_slice_in_dim(result, value, mine, 1)
    return lax.dynamic_update_slice_in_dim(result, other, value.shape[1] - mine, 1)


def own_channels(terms):
    members = lax.axis_size("tp")
    if members != 2:
        return lax.psum_scatter(terms, "tp", scatter_dimension=1, tiled=True).astype(jnp.float32)
    width = terms.shape[1] // 2
    mine = lax.axis_index("tp") * width
    other = swapped(lax.dynamic_slice_in_dim(terms, width - mine, width, 1), "tp", members)
    own = lax.dynamic_slice_in_dim(terms, mine, width, 1)
    return own.astype(jnp.float32) + other.astype(jnp.float32)


def body(
    resid,
    query_one,
    key_one,
    query_two,
    key_two,
    values,
    mix_lambda,
    segments,
    head_gain,
    out_weight,
    mixer_gain,
    gate_weight,
    up_weight,
    down_weight,
):
    rows = query_one.shape[0]
    heads = mix_lambda.shape[0]
    position = lax.axis_index("sp")
    both_all, down_all = gathered(gate_weight, up_weight, down_weight)
    carried = (key_one, key_two, values, segments)
    earlier = [carried]
    for step in range(REACH):
        carried = shifted((carried[0], carried[1], carried[2], carried[3]), "sp", 1)
        earlier.insert(0, carried)
    width = (REACH + 1) * rows
    k_first = jnp.concatenate([piece[0] for piece in earlier], 0).reshape(width, heads, HD)
    k_second = jnp.concatenate([piece[1] for piece in earlier], 0).reshape(width, heads, HD)
    vals = jnp.concatenate([piece[2] for piece in earlier], 0).reshape(width, heads, VD)
    seg_key = jnp.concatenate([piece[3] for piece in earlier], 0)
    q_pos = position * rows + jnp.arange(rows, dtype=jnp.int32)
    k_pos = (position - REACH) * rows + jnp.arange(width, dtype=jnp.int32)
    allowed = (
        (seg_key[None, :] == segments[:, None])
        & (k_pos[None, :] <= q_pos[:, None])
        & (k_pos[None, :] >= 0)
    )

    def weights(query, keys):
        score = jnp.einsum(
            "qhd,khd->hqk", query.reshape(rows, heads, HD), keys, preferred_element_type=jnp.float32
        ) * HD ** (-0.5)
        score = jnp.where(allowed[None], score, -jnp.inf)
        score = score - jnp.max(score, axis=-1, keepdims=True)
        expo = jnp.exp(score)
        return (expo / jnp.sum(expo, axis=-1, keepdims=True)).astype(jnp.bfloat16)

    out_first = jnp.einsum(
        "hqk,khe->qhe", weights(query_one, k_first), vals, preferred_element_type=jnp.float32
    )
    out_second = jnp.einsum(
        "hqk,khe->qhe", weights(query_two, k_second), vals, preferred_element_type=jnp.float32
    )
    head_out = out_first - mix_lambda[None, :, None] * out_second
    meansq = jnp.mean(head_out * head_out, axis=-1, keepdims=True)
    attn_rows = (
        (head_out * lax.rsqrt(meansq + 1e-05) * head_gain)
        .reshape(rows, heads * VD)
        .astype(jnp.bfloat16)
    )
    projected = jnp.dot(
        whole_channels(attn_rows),
        out_weight,
        preferred_element_type=jnp.float32,
    )
    mid = (resid.astype(jnp.float32) + projected).astype(jnp.bfloat16)
    midf = mid.astype(jnp.float32)
    squares = lax.psum(jnp.sum(midf * midf, axis=1), "tp")
    channels = mid.shape[1] * lax.axis_size("tp")
    normed = (midf * lax.rsqrt(squares / channels + 1e-06)[:, None] * mixer_gain).astype(
        jnp.bfloat16
    )
    members = lax.axis_size("sp")
    paired = len(groups(members)[0][0]) == 2
    if paired:
        normed = jnp.concatenate([normed, swapped(normed, "sp", members)], 0)
    whole_rows = whole_channels(normed)
    whole_rows, both_all, down_all = lax.optimization_barrier((whole_rows, both_all, down_all))
    part = both_all.shape[1] // 2
    gate = jnp.dot(whole_rows, both_all[:, :part], preferred_element_type=jnp.float32)
    up = jnp.dot(whole_rows, both_all[:, part:], preferred_element_type=jnp.float32)
    hidden = (jax.nn.silu(gate) * up).astype(jnp.bfloat16)
    terms = jnp.dot(hidden, down_all, preferred_element_type=jnp.float32)
    summed = own_channels(terms.astype(jnp.bfloat16))
    if paired:
        came = swapped(summed[rows:].astype(jnp.bfloat16), "sp", members)
        summed = summed[:rows] + came.astype(jnp.float32)
    return (midf + summed).astype(jnp.bfloat16)


def rdma(src, dst, send, recv, device):
    return pltpu.make_async_remote_copy(
        src_ref=src, dst_ref=dst, send_sem=send, recv_sem=recv,
        device_id=device, device_id_type=pl.DeviceIdType.MESH,
    )


def layer_kernel(
    plane, lines, sub, pieces,
    resid, q_one, k_one, q_two, k_two, vals, lam, seg, head_gain, out_w, mix_gain, gate, up, down,
    out,
    qb, kb, vb, sb, ao, ar, oww, res, mid, mg, xa, ga, ua, da, hid, pown, psend, precv, csend, crecv,
    s_qkv, r_qkv, s_halo, r_halo, s_w1, s_w2, s_relay, r_w, s_ao, r_ao, s_pair, r_pair,
    s_ag, r_ag, s_xd, r_xd, s_pp, r_pp, s_ch, r_ch, s_loc,
):
    sp, tp = lax.axis_index("sp"), lax.axis_index("tp")
    z, p = lax.div(sp, plane), lax.rem(sp, plane)
    rows, half = resid.shape
    heads = plane
    depth = gate.shape[0]
    units = gate.shape[1] // lines
    own_rows = plane * rows
    px, py = lax.rem(p, 2), lax.div(p, 2)

    def peer(k):
        a, b = k % 2, k // 2
        return (py + b - 2 * py * b) * 2 + px + a - 2 * px * a

    def line_peer(d):
        return lax.rem(z + d, lines)

    partner = (sp, 1 - tp)
    in_plane = [peer(k) for k in range(1, plane)]

    barrier = pltpu.get_barrier_semaphore()
    for q in in_plane:
        pl.semaphore_signal(barrier, inc=1, device_id=(z * plane + q, tp), device_id_type=pl.DeviceIdType.MESH)
    for d in range(1, lines):
        pl.semaphore_signal(barrier, inc=1, device_id=(line_peer(d) * plane + p, tp), device_id_type=pl.DeviceIdType.MESH)
    pl.semaphore_signal(barrier, inc=1, device_id=partner, device_id_type=pl.DeviceIdType.MESH)
    pl.semaphore_wait(barrier, plane - 1 + lines - 1 + 1)

    sources = (k_one, k_two, vals, q_one, q_two)

    def mul(i, n):
        return pl.multiple_of(i * n, n)

    def qkv_src(a, head):
        wide = VD if a == 2 else HD
        return sources[a].at[:, pl.ds(mul(head, wide), wide)]

    def kv_dst(a, block):
        at = pl.ds(mul(block, rows), rows)
        if a == 2:
            return vb.at[at, :]
        return kb.at[a, at, :]

    def qkv_dst(a, block):
        if a == 5:
            return sb.at[plane + block]
        if a < 3:
            return kv_dst(a, plane + block)
        return qb.at[a - 3, pl.ds(mul(block, rows), rows), :]

    def qkv_copy(k, a):
        q = in_plane[k]
        src = seg if a == 5 else qkv_src(a, q)
        return rdma(src, qkv_dst(a, p), s_qkv.at[k, a], r_qkv.at[p, a], (z * plane + q, tp))

    def halo_copy(block, a, own):
        if a == 3:
            src = seg if own else sb.at[plane + block]
            dst = sb.at[block]
        else:
            src = qkv_src(a, p) if own else kv_dst(a, plane + block)
            dst = kv_dst(a, block)
        return rdma(src, dst, s_halo.at[block, a], r_halo.at[block, a], (sp + plane, tp))

    def weight_dst(s, a):
        if a == 0:
            return ga.at[pl.ds(mul(s, depth), depth), :]
        if a == 1:
            return ua.at[pl.ds(mul(s, depth), depth), :]
        return da.at[:, pl.ds(mul(s, depth), depth)]

    def weight_src(line, a):
        at = pl.ds(mul(line, units), units)
        if a == 0:
            return gate.at[:, at]
        if a == 1:
            return up.at[:, at]
        return down.at[at, :]

    def w1_copy(d, a):
        zz = line_peer(d)
        return rdma(weight_src(zz, a), weight_dst(sp, a), s_w1.at[d - 1, a], r_w.at[sp, a], (zz * plane + p, tp))

    def w2_copy(k, d, a):
        s = line_peer(d) * plane + p
        src = weight_src(z, a) if d == 0 else weight_dst(s, a)
        return rdma(src, weight_dst(s, a), s_w2.at[k - 1, d, a], r_w.at[s, a], (z * plane + peer(k), tp))

    def relay_copy(d, a):
        k = 1 + (d + a) % 2
        s = line_peer(d) * plane + peer(k)
        return rdma(weight_dst(s, a), weight_dst(s, a), s_relay.at[d, a], r_w.at[s, a], (z * plane + peer(3 - k), tp))

    def weight_arrived(d, a, q):
        s = line_peer(d) * plane + q
        arrived(weight_dst(s, a), r_w.at[s, a])

    def spread(d, a):
        if d > 0:
            weight_arrived(d, a, p)
        for k in (1, 2):
            w2_copy(k, d, a).start()

    def relay(d, a):
        weight_arrived(d, a, peer(1 + (d + a) % 2))
        relay_copy(d, a).start()

    def rest_of_weights(a):
        for d in range(lines):
            weight_arrived(d, a, peer(2 - (d + a) % 2))
            weight_arrived(d, a, peer(3))

    def arrived(dst, sem):
        rdma(dst, dst, s_pair.at[0], sem, partner).wait_recv()

    def local(src, dst, i):
        return pltpu.make_async_copy(src, dst, s_loc.at[i])

    for a in (0, 1, 2, 5):
        for k in range(plane - 1):
            qkv_copy(k, a).start()
    for k in range(plane - 1):
        for a in (3, 4):
            qkv_copy(k, a).start()

    @pl.when(z < lines - 1)
    def _():
        for a in range(4):
            halo_copy(p, a, True).start()

    for a in range(3):
        for d in range(1, lines):

            @pl.when(line_peer(d) < z)
            def _():
                w1_copy(d, a).start()

    locals_ = [local(qkv_src(a, p), qkv_dst(a, p), a) for a in range(5)]
    locals_.append(local(out_w, oww, 5))
    locals_.append(local(resid, res, 6))
    for a in range(3):
        locals_.append(local(weight_src(z, a), weight_dst(sp, a), 7 + a))
    for c in locals_:
        c.start()
    sb[plane + p] = seg[...]
    mg[tp] = mix_gain[...]
    rdma(mix_gain, mg.at[tp], s_pair.at[0], r_pair.at[0], partner).start()

    for a in range(2):
        spread(0, a)

    @pl.when(z == 0)
    def _():
        vb[: plane * rows, :] = jnp.zeros((plane * rows, VD), vb.dtype)
        kb[:, : plane * rows, :] = jnp.zeros((2, plane * rows, HD), kb.dtype)
        for b in range(plane):
            sb[b] = jnp.full(sb.shape[1:], -1, sb.dtype)

    nearest = jnp.maximum(peer(1), peer(2))
    other = jnp.minimum(peer(1), peer(2))
    for q in (nearest, jnp.maximum(other, peer(3)), jnp.minimum(other, peer(3))):
        for a in (0, 1, 2, 5):
            arrived(qkv_dst(a, q), r_qkv.at[q, a])

        @pl.when(z < lines - 1)
        def _():
            for a in range(4):
                halo_copy(q, a, False).start()

    for k in range(plane - 1):
        q = in_plane[k]
        for a in (3, 4):
            arrived(qkv_dst(a, q), r_qkv.at[q, a])
    for c in locals_[:5]:
        c.wait()

    scale = HD ** (-0.5) * 1.4426950408889634
    window = (REACH + 1) * rows

    def ao_remote(j):
        at = pl.ds(mul(tp * heads + p, VD), VD)
        return rdma(ao.at[j], ar.at[:, at], s_ao.at[j], r_ao.at[p], (z * plane + j, tp))

    def ao_local(j):
        at = pl.ds(mul(tp * heads + p, VD), VD)
        return local(ao.at[j], ar.at[:, at], 10)

    coef = lam[p]

    def query_block(i, carry):
        j = plane - 1 - i

        @pl.when(z > 0)
        def _():
            for a in range(3):
                arrived(kv_dst(a, j), r_halo.at[j, a])
            arrived(sb.at[j], r_halo.at[j, 3])

        for a in range(3):
            for d in range(1, lines):

                @pl.when((i == plane - 1) & (line_peer(d) > z))
                def _():
                    w1_copy(d, a).start()

        at = pl.ds(mul(j, rows), window)
        key_seg = jnp.concatenate([sb[j + n] for n in range(REACH + 1)], axis=1).astype(jnp.float32)
        own_seg = jnp.broadcast_to(sb[plane + j].astype(jnp.float32), (128, rows))
        seg_col = jnp.transpose(own_seg)[:, :1]
        for u in range(rows // sub):
            col = lax.broadcasted_iota(jnp.int32, (sub, window), 1)
            row = lax.broadcasted_iota(jnp.int32, (sub, window), 0) + (REACH * rows + u * sub)
            ok = (key_seg == seg_col[u * sub : (u + 1) * sub]) & (col <= row)
            outs = []
            for m in range(2):
                q = qb[m, pl.ds(pl.multiple_of(j * rows + u * sub, sub), sub), :]
                s = lax.dot_general(
                    q, kb[m, at, :], (((1,), (1,)), ((), ())), preferred_element_type=jnp.float32
                )
                s = jnp.where(ok, s, -1e30)
                top = jnp.max(s, axis=1, keepdims=True)
                e = jnp.exp2((s - top) * scale)
                total = jnp.sum(e, axis=1, keepdims=True)
                o = jnp.dot(e.astype(jnp.bfloat16), vb[at, :], preferred_element_type=jnp.float32)
                outs.append(o / total)
            h = outs[0] - coef * outs[1]
            ms = jnp.mean(h * h, axis=1, keepdims=True)
            h = h * lax.rsqrt(ms + 1e-05) * head_gain[...]
            ao[j, pl.ds(u * sub, sub), :] = h.astype(ao.dtype)

        @pl.when(j != p)
        def _():
            ao_remote(j).start()

        @pl.when(j == p)
        def _():
            ao_local(j).start()

        return carry

    lax.fori_loop(0, plane, query_block, 0)
    spread(0, 2)
    relay(0, 0)
    relay(0, 1)

    ao_local(p).wait()
    for q in in_plane:
        at = pl.ds(mul(tp * heads + q, VD), VD)
        arrived(ar.at[:, at], r_ao.at[q])
    mine = pl.ds(mul(tp, half), half)
    theirs = pl.ds(mul(1 - tp, half), half)
    swap = rdma(ar.at[:, mine], ar.at[:, mine], s_pair.at[1], r_pair.at[1], partner)
    swap.start()
    for c in locals_[5:7]:
        c.wait()
    acc = jnp.dot(ar[:, mine], oww[mine, :], preferred_element_type=jnp.float32)
    arrived(ar.at[:, theirs], r_pair.at[1])
    acc = acc + jnp.dot(ar[:, theirs], oww[theirs, :], preferred_element_type=jnp.float32)
    mid[tp] = (res[...].astype(jnp.float32) + acc).astype(mid.dtype)
    swap_mid = rdma(mid.at[tp], mid.at[tp], s_pair.at[2], r_pair.at[2], partner)
    swap_mid.start()
    arrived(mid.at[1 - tp], r_pair.at[2])
    arrived(mg.at[1 - tp], r_pair.at[0])
    m0, m1 = mid[0].astype(jnp.float32), mid[1].astype(jnp.float32)
    squares = jnp.sum(m0 * m0, axis=1, keepdims=True) + jnp.sum(m1 * m1, axis=1, keepdims=True)
    inv = lax.rsqrt(squares / (2 * half) + 1e-06)
    xa[z, 0] = (m0 * inv * mg[0]).astype(xa.dtype)
    xa[z, 1] = (m1 * inv * mg[1]).astype(xa.dtype)

    piece = rows // pieces

    def ag_copy(b, to, c):
        ref = xa.at[b, tp, pl.ds(c * piece, piece), :]
        return rdma(ref, ref, s_ag.at[b, to, c], r_ag.at[b, c], (sp + plane * (2 * to - 1), tp))

    def xd_copy(b):
        return rdma(xa.at[b, tp], xa.at[b, tp], s_xd.at[b], r_xd.at[b], partner)

    for c in range(pieces):

        @pl.when(z < lines - 1)
        def _():
            ag_copy(z, 1, c).start()

        @pl.when(z > 0)
        def _():
            ag_copy(z, 0, c).start()

    def from_above(d):
        above = z + d

        @pl.when(above < lines)
        def _():
            for c in range(pieces):
                arrived(xa.at[above, tp, pl.ds(c * piece, piece), :], r_ag.at[above, c])

                @pl.when(z > 0)
                def _():
                    ag_copy(above, 0, c).start()

            xd_copy(above).start()

    def from_below(d):
        below = z - d

        @pl.when(below >= 0)
        def _():
            for c in range(pieces):
                arrived(xa.at[below, tp, pl.ds(c * piece, piece), :], r_ag.at[below, c])

                @pl.when(z < lines - 1)
                def _():
                    ag_copy(below, 1, c).start()

            xd_copy(below).start()

    tile = units // 3

    def hidden_block(b):
        @pl.when(b != z)
        def _():
            arrived(xa.at[b, 1 - tp], r_xd.at[b])

        def hidden_tile(u, carry):
            at = pl.ds(mul(u, tile), tile)
            g = jnp.dot(xa[b, 0], ga[:half, at], preferred_element_type=jnp.float32)
            g = g + jnp.dot(xa[b, 1], ga[half:, at], preferred_element_type=jnp.float32)
            v = jnp.dot(xa[b, 0], ua[:half, at], preferred_element_type=jnp.float32)
            v = v + jnp.dot(xa[b, 1], ua[half:, at], preferred_element_type=jnp.float32)
            hid[b, :, at] = (g / (1.0 + jnp.exp(-g)) * v).astype(hid.dtype)
            return carry

        lax.fori_loop(0, units // tile, hidden_tile, 0)

    def next_block(i):
        upper = lines - 1 - z
        return jnp.where(i < upper, z + 1 + i, z - 1 - (i - upper))

    for d in range(1, lines):
        spread(d, 0)
    relay(0, 2)
    for d in range(1, lines):
        spread(d, 1)
    for d in range(1, lines):
        relay(d, 0)
    from_above(1)
    for d in range(1, lines):
        relay(d, 1)
        spread(d, 2)
    from_above(2)
    from_below(1)
    for c in locals_[7:]:
        c.wait()
    rest_of_weights(0)
    rest_of_weights(1)
    hidden_block(z)
    for d in range(1, lines):
        relay(d, 2)
    hidden_block(next_block(0))
    from_below(2)

    def rank(zz):
        far = list(range(2, lines)) + [1]
        back = [lines - 1 - b for b in far]
        travel = [
            (far.index(b) + zz if b > zz else back.index(b) + lines - 1 - zz, b) for b in range(lines) if b != zz
        ]
        return [b for _, b in sorted(travel)] + [zz]

    def order(i):
        b = rank(0)[i]
        for zz in range(1, lines):
            b = jnp.where(z == zz, rank(zz)[i], b)
        return b

    wide = half // 2

    def down_block(b):
        def down_tile(c, carry):
            theirs_at = pl.ds(pl.multiple_of((1 - tp) * half + c * wide, wide), wide)
            own_at = pl.ds(pl.multiple_of(tp * half + c * wide, wide), wide)
            at = pl.ds(mul(c, wide), wide)
            o = jnp.dot(hid[b], da[:, theirs_at], preferred_element_type=jnp.float32)
            psend[b, :, at] = o.astype(psend.dtype)
            o = jnp.dot(hid[b], da[:, own_at], preferred_element_type=jnp.float32)
            pown[b, :, at] = o
            return carry

        lax.fori_loop(0, half // wide, down_tile, 0)
        rdma(psend.at[b], precv.at[b], s_pp.at[b], r_pp.at[b], partner).start()

    def chain_copy(b, to, c):
        near = jnp.where(b == z + 1, lines, b) if to == 1 else b
        at = pl.ds(c * piece, piece)
        return rdma(
            csend.at[b, at, :], crecv.at[near, at, :], s_ch.at[b, c], r_ch.at[near, c],
            (sp + plane * (2 * to - 1), tp),
        )

    def chain(b):
        arrived(precv.at[b], r_pp.at[b])
        incoming = ((b < z) & (z < lines - 1)) | ((b > z) & (z > 0))
        for c in range(pieces):
            at = pl.ds(c * piece, piece)

            @pl.when(incoming)
            def _():
                arrived(crecv.at[b, at, :], r_ch.at[b, c])
                own = pown[b, at, :] + precv[b, at, :].astype(jnp.float32)
                csend[b, at, :] = (own + crecv[b, at, :].astype(jnp.float32)).astype(csend.dtype)

            @pl.when(jnp.logical_not(incoming))
            def _():
                own = pown[b, at, :] + precv[b, at, :].astype(jnp.float32)
                csend[b, at, :] = own.astype(csend.dtype)

            @pl.when(b > z)
            def _():
                chain_copy(b, 1, c).start()

            @pl.when(b < z)
            def _():
                chain_copy(b, 0, c).start()

    at_end = (z == 0) | (z == lines - 1)

    @pl.when(at_end)
    def _():
        hidden_block(next_block(1))
        rest_of_weights(2)
        down_block(order(0))
        chain(order(0))
        for i in range(1, lines - 2):
            from_above(i + 2)
            from_below(i + 2)
            hidden_block(next_block(i + 1))
            down_block(order(i))
            chain(order(i))
        down_block(order(lines - 2))
        chain(order(lines - 2))
        down_block(z)

    @pl.when(jnp.logical_not(at_end))
    def _():
        for i in range(3, lines):
            from_above(i)
            from_below(i)
        for i in range(1, lines - 1):
            hidden_block(next_block(i))
        rest_of_weights(2)
        for i in range(lines):
            down_block(order(i))
        for i in range(lines - 1):
            chain(order(i))

    arrived(precv.at[z], r_pp.at[z])
    pown[z] = pown[z] + precv[z].astype(jnp.float32) + mid[tp].astype(jnp.float32)
    for c in range(pieces):
        at = pl.ds(c * piece, piece)

        @pl.when(z < lines - 1)
        def _():
            arrived(crecv.at[z, at, :], r_ch.at[z, c])
            pown[z, at, :] = pown[z, at, :] + crecv[z, at, :].astype(jnp.float32)

        @pl.when(z > 0)
        def _():
            arrived(crecv.at[lines, at, :], r_ch.at[lines, c])
            pown[z, at, :] = pown[z, at, :] + crecv[lines, at, :].astype(jnp.float32)

        out[at, :] = pown[z, at, :].astype(out.dtype)

    for k in range(plane - 1):
        for a in range(6):
            qkv_copy(k, a).wait_send()
    for d in range(lines):
        for a in range(3):
            w2_copy(1, d, a).wait_send()
            w2_copy(2, d, a).wait_send()
            relay_copy(d, a).wait_send()
    for d in range(1, lines):
        for a in range(3):
            w1_copy(d, a).wait_send()

    @pl.when(z < lines - 1)
    def _():
        for a in range(4):
            halo_copy(p, a, True).wait_send()
            for q in in_plane:
                halo_copy(q, a, False).wait_send()

    for q in in_plane:
        ao_remote(q).wait_send()
    rdma(mix_gain, mg.at[tp], s_pair.at[0], r_pair.at[0], partner).wait_send()
    swap.wait_send()
    swap_mid.wait_send()
    for b in range(lines):
        rdma(psend.at[b], precv.at[b], s_pp.at[b], r_pp.at[b], partner).wait_send()

        @pl.when(b != z)
        def _():
            xd_copy(b).wait_send()

        @pl.when((b <= z) & (z < lines - 1))
        def _():
            for c in range(pieces):
                ag_copy(b, 1, c).wait_send()

        @pl.when((b >= z) & (z > 0))
        def _():
            for c in range(pieces):
                ag_copy(b, 0, c).wait_send()

        @pl.when(b > z)
        def _():
            for c in range(pieces):
                chain_copy(b, 1, c).wait_send()

        @pl.when(b < z)
        def _():
            for c in range(pieces):
                chain_copy(b, 0, c).wait_send()


def fast_body(resid, query_one, key_one, query_two, key_two, values, mix_lambda, segments, head_gain,
              out_weight, mixer_gain, gate_weight, up_weight, down_weight):
    plane = mix_lambda.shape[0]
    lines = lax.axis_size("sp") // plane
    rows, half = resid.shape
    depth, units = gate_weight.shape[0], gate_weight.shape[1] // lines
    full = depth * plane * lines
    bf, f32 = jnp.bfloat16, jnp.float32
    sub = rows // 3
    pieces = 2
    dma = pltpu.SemaphoreType.DMA
    anywhere = pl.BlockSpec(memory_space=pl.ANY)
    vmem = pl.BlockSpec(memory_space=pltpu.VMEM)
    smem = pl.BlockSpec(memory_space=pltpu.SMEM)
    flops = 6 * rows * plane * full * units + 2 * rows * full * half + 24 * rows * plane * rows * 5 * VD
    return pl.pallas_call(
        functools.partial(layer_kernel, plane, lines, sub, pieces),
        out_shape=jax.ShapeDtypeStruct((rows, half), bf),
        in_specs=[anywhere] * 6 + [smem, vmem, vmem, anywhere, vmem, anywhere, anywhere, anywhere],
        out_specs=vmem,
        scratch_shapes=[
            pltpu.VMEM((2, plane * rows, HD), bf),
            pltpu.VMEM((2, 2 * plane * rows, HD), bf),
            pltpu.VMEM((2 * plane * rows, VD), bf),
            pltpu.VMEM((2 * plane, 1, rows), jnp.int32),
            pltpu.VMEM((plane, rows, VD), bf),
            pltpu.VMEM((rows, full), bf),
            pltpu.VMEM((full, half), bf),
            pltpu.VMEM((rows, half), bf),
            pltpu.VMEM((2, rows, half), bf),
            pltpu.VMEM((2, 1, half), f32),
            pltpu.VMEM((lines, 2, rows, half), bf),
            pltpu.VMEM((full, units), bf),
            pltpu.VMEM((full, units), bf),
            pltpu.VMEM((units, full), bf),
            pltpu.VMEM((lines, rows, units), bf),
            pltpu.VMEM((lines, rows, half), f32),
            pltpu.VMEM((lines, rows, half), bf),
            pltpu.VMEM((lines, rows, half), bf),
            pltpu.VMEM((lines, rows, half), bf),
            pltpu.VMEM((lines + 1, rows, half), bf),
            dma((plane - 1, 6)), dma((plane, 6)),
            dma((plane, 4)), dma((plane, 4)),
            dma((lines - 1, 3)), dma((2, lines, 3)), dma((lines, 3)), dma((plane * lines, 3)),
            dma((plane,)), dma((plane,)),
            dma((3,)), dma((3,)),
            dma((lines, 2, pieces)), dma((lines, pieces)),
            dma((lines,)), dma((lines,)),
            dma((lines,)), dma((lines,)),
            dma((lines, pieces)), dma((lines + 1, pieces)),
            dma((11,)),
        ],
        compiler_params=pltpu.CompilerParams(
            collective_id=0, has_side_effects=True, vmem_limit_bytes=60 * 1024 * 1024
        ),
        cost_estimate=pl.CostEstimate(flops=flops, bytes_accessed=2 * full * units, transcendentals=0),
        name="layer",
    )(resid, query_one, key_one, query_two, key_two, values, mix_lambda, segments.reshape(1, rows),
      head_gain.reshape(1, VD), out_weight, mixer_gain.reshape(1, half), gate_weight, up_weight, down_weight)


def fits(mesh):
    sp, tp = mesh.shape["sp"], mesh.shape["tp"]
    return tp == 2 and sp % (REACH * 2) == 0


def choose(mesh):
    def step(*args):
        heads = args[6].shape[0]
        if fits(mesh) and heads == REACH:
            return fast_body(*args)
        return body(*args)

    return step


def solution(mesh):
    in_specs = (
        P("sp", "tp"),
        P("sp", "tp"),
        P("sp", "tp"),
        P("sp", "tp"),
        P("sp", "tp"),
        P("sp", "tp"),
        P("tp"),
        P("sp"),
        P(),
        P(None, "tp"),
        P("tp"),
        P("sp", "tp"),
        P("sp", "tp"),
        P("tp", "sp"),
    )
    out_specs = P("sp", "tp")
    return jax.shard_map(choose(mesh), mesh=mesh, in_specs=in_specs, out_specs=out_specs, check_vma=False)
```

```python
import functools

import jax
import jax.numpy as jnp
from jax import lax
from jax.experimental import pallas as pl
from jax.experimental.pallas import tpu as pltpu
from jax.sharding import PartitionSpec as P

HD = 128
VD = 256
REACH = 4
SHARE = 2


def shifted(value, axis, by):
    length = lax.axis_size(axis)
    pairs = [(i, i + by) for i in range(length) if 0 <= i + by < length]
    return lax.ppermute(value, axis, pairs)


def groups(length):
    share = SHARE if length % SHARE == 0 else 1
    plane = [[i * share + j for j in range(share)] for i in range(length // share)]
    across = [[i * share + j for i in range(length // share)] for j in range(share)]
    return plane, across


def spread(blocks):
    length = lax.axis_size("sp")
    share = blocks.shape[0]
    if share == 1:
        return blocks
    mine = lax.rem(lax.axis_index("sp"), share)
    own = lax.dynamic_index_in_dim(blocks, mine, 0, keepdims=True)
    result = lax.dynamic_update_slice_in_dim(jnp.zeros_like(blocks), own, mine, 0)
    for by in range(1, share):
        pairs = [(i, i - i % share + (i + by) % share) for i in range(length)]
        sent = lax.dynamic_index_in_dim(blocks, lax.rem(mine + by, share), 0, keepdims=True)
        came = lax.ppermute(sent, "sp", pairs)
        result = lax.dynamic_update_slice_in_dim(result, came, lax.rem(mine + share - by, share), 0)
    return result


def gathered(gate_weight, up_weight, down_weight):
    plane, across = groups(lax.axis_size("sp"))
    share = len(plane[0])
    depth, units = gate_weight.shape
    part = units // share
    both = [gate_weight.reshape(depth, share, part), up_weight.reshape(depth, share, part)]
    both = jnp.concatenate(both, 2).transpose(1, 0, 2)
    both = spread(both).reshape(share * depth, 2 * part)
    down = spread(down_weight.reshape(share, part, depth))
    down = down.transpose(1, 0, 2).reshape(part, share * depth)
    both = lax.all_gather(both, "sp", axis=0, tiled=True, axis_index_groups=across)
    down = lax.all_gather(down, "sp", axis=1, tiled=True, axis_index_groups=across)
    return both, down


def swapped(value, axis, members):
    return lax.ppermute(value, axis, [(i, i ^ 1) for i in range(members)])


def whole_channels(value):
    members = lax.axis_size("tp")
    if members != 2:
        return lax.all_gather(value, "tp", axis=1, tiled=True)
    other = swapped(value, "tp", members)
    mine = lax.axis_index("tp") * value.shape[1]
    result = jnp.zeros((value.shape[0], 2 * value.shape[1]), value.dtype)
    result = lax.dynamic_update_slice_in_dim(result, value, mine, 1)
    return lax.dynamic_update_slice_in_dim(result, other, value.shape[1] - mine, 1)


def own_channels(terms):
    members = lax.axis_size("tp")
    if members != 2:
        return lax.psum_scatter(terms, "tp", scatter_dimension=1, tiled=True).astype(jnp.float32)
    width = terms.shape[1] // 2
    mine = lax.axis_index("tp") * width
    other = swapped(lax.dynamic_slice_in_dim(terms, width - mine, width, 1), "tp", members)
    own = lax.dynamic_slice_in_dim(terms, mine, width, 1)
    return own.astype(jnp.float32) + other.astype(jnp.float32)


def body(
    resid,
    query_one,
    key_one,
    query_two,
    key_two,
    values,
    mix_lambda,
    segments,
    head_gain,
    out_weight,
    mixer_gain,
    gate_weight,
    up_weight,
    down_weight,
):
    rows = query_one.shape[0]
    heads = mix_lambda.shape[0]
    position = lax.axis_index("sp")
    both_all, down_all = gathered(gate_weight, up_weight, down_weight)
    carried = (key_one, key_two, values, segments)
    earlier = [carried]
    for step in range(REACH):
        carried = shifted((carried[0], carried[1], carried[2], carried[3]), "sp", 1)
        earlier.insert(0, carried)
    width = (REACH + 1) * rows
    k_first = jnp.concatenate([piece[0] for piece in earlier], 0).reshape(width, heads, HD)
    k_second = jnp.concatenate([piece[1] for piece in earlier], 0).reshape(width, heads, HD)
    vals = jnp.concatenate([piece[2] for piece in earlier], 0).reshape(width, heads, VD)
    seg_key = jnp.concatenate([piece[3] for piece in earlier], 0)
    q_pos = position * rows + jnp.arange(rows, dtype=jnp.int32)
    k_pos = (position - REACH) * rows + jnp.arange(width, dtype=jnp.int32)
    allowed = (
        (seg_key[None, :] == segments[:, None])
        & (k_pos[None, :] <= q_pos[:, None])
        & (k_pos[None, :] >= 0)
    )

    def weights(query, keys):
        score = jnp.einsum(
            "qhd,khd->hqk", query.reshape(rows, heads, HD), keys, preferred_element_type=jnp.float32
        ) * HD ** (-0.5)
        score = jnp.where(allowed[None], score, -jnp.inf)
        score = score - jnp.max(score, axis=-1, keepdims=True)
        expo = jnp.exp(score)
        return (expo / jnp.sum(expo, axis=-1, keepdims=True)).astype(jnp.bfloat16)

    out_first = jnp.einsum(
        "hqk,khe->qhe", weights(query_one, k_first), vals, preferred_element_type=jnp.float32
    )
    out_second = jnp.einsum(
        "hqk,khe->qhe", weights(query_two, k_second), vals, preferred_element_type=jnp.float32
    )
    head_out = out_first - mix_lambda[None, :, None] * out_second
    meansq = jnp.mean(head_out * head_out, axis=-1, keepdims=True)
    attn_rows = (
        (head_out * lax.rsqrt(meansq + 1e-05) * head_gain)
        .reshape(rows, heads * VD)
        .astype(jnp.bfloat16)
    )
    projected = jnp.dot(
        whole_channels(attn_rows),
        out_weight,
        preferred_element_type=jnp.float32,
    )
    mid = (resid.astype(jnp.float32) + projected).astype(jnp.bfloat16)
    midf = mid.astype(jnp.float32)
    squares = lax.psum(jnp.sum(midf * midf, axis=1), "tp")
    channels = mid.shape[1] * lax.axis_size("tp")
    normed = (midf * lax.rsqrt(squares / channels + 1e-06)[:, None] * mixer_gain).astype(
        jnp.bfloat16
    )
    members = lax.axis_size("sp")
    paired = len(groups(members)[0][0]) == 2
    if paired:
        normed = jnp.concatenate([normed, swapped(normed, "sp", members)], 0)
    whole_rows = whole_channels(normed)
    whole_rows, both_all, down_all = lax.optimization_barrier((whole_rows, both_all, down_all))
    part = both_all.shape[1] // 2
    gate = jnp.dot(whole_rows, both_all[:, :part], preferred_element_type=jnp.float32)
    up = jnp.dot(whole_rows, both_all[:, part:], preferred_element_type=jnp.float32)
    hidden = (jax.nn.silu(gate) * up).astype(jnp.bfloat16)
    terms = jnp.dot(hidden, down_all, preferred_element_type=jnp.float32)
    summed = own_channels(terms.astype(jnp.bfloat16))
    if paired:
        came = swapped(summed[rows:].astype(jnp.bfloat16), "sp", members)
        summed = summed[:rows] + came.astype(jnp.float32)
    return (midf + summed).astype(jnp.bfloat16)


def rdma(src, dst, send, recv, device):
    return pltpu.make_async_remote_copy(
        src_ref=src, dst_ref=dst, send_sem=send, recv_sem=recv,
        device_id=device, device_id_type=pl.DeviceIdType.MESH,
    )


def layer_kernel(
    plane, lines, sub, pieces,
    resid, q_one, k_one, q_two, k_two, vals, lam, seg, head_gain, out_w, mix_gain, gate, up, down,
    out,
    qb, kb, vb, sb, ao, ar, oww, res, mid, mg, xa, ga, ua, da, hid, pown, psend, precv, csend, crecv,
    s_qkv, r_qkv, s_halo, r_halo, s_w1, s_w2, s_relay, r_w, s_ao, r_ao, s_pair, r_pair,
    s_ag, r_ag, s_xd, r_xd, s_pp, r_pp, s_ch, r_ch, s_loc,
):
    sp, tp = lax.axis_index("sp"), lax.axis_index("tp")
    z, p = lax.div(sp, plane), lax.rem(sp, plane)
    rows, half = resid.shape
    heads = plane
    depth = gate.shape[0]
    units = gate.shape[1] // lines
    own_rows = plane * rows
    px, py = lax.rem(p, 2), lax.div(p, 2)

    def peer(k):
        a, b = k % 2, k // 2
        return (py + b - 2 * py * b) * 2 + px + a - 2 * px * a

    def line_peer(d):
        return lax.rem(z + d, lines)

    partner = (sp, 1 - tp)
    in_plane = [peer(k) for k in range(1, plane)]

    barrier = pltpu.get_barrier_semaphore()
    for q in in_plane:
        pl.semaphore_signal(barrier, inc=1, device_id=(z * plane + q, tp), device_id_type=pl.DeviceIdType.MESH)
    for d in range(1, lines):
        pl.semaphore_signal(barrier, inc=1, device_id=(line_peer(d) * plane + p, tp), device_id_type=pl.DeviceIdType.MESH)
    pl.semaphore_signal(barrier, inc=1, device_id=partner, device_id_type=pl.DeviceIdType.MESH)
    pl.semaphore_wait(barrier, plane - 1 + lines - 1 + 1)

    sources = (k_one, k_two, vals, q_one, q_two)

    def mul(i, n):
        return pl.multiple_of(i * n, n)

    def qkv_src(a, head):
        wide = VD if a == 2 else HD
        return sources[a].at[:, pl.ds(mul(head, wide), wide)]

    def kv_dst(a, block):
        at = pl.ds(mul(block, rows), rows)
        if a == 2:
            return vb.at[at, :]
        return kb.at[a, at, :]

    def qkv_dst(a, block):
        if a == 5:
            return sb.at[plane + block]
        if a < 3:
            return kv_dst(a, plane + block)
        return qb.at[a - 3, pl.ds(mul(block, rows), rows), :]

    def qkv_copy(k, a):
        q = in_plane[k]
        src = sb.at[plane + p] if a == 5 else qkv_src(a, q)
        return rdma(src, qkv_dst(a, p), s_qkv.at[k, a], r_qkv.at[p, a], (z * plane + q, tp))

    def halo_copy(block, a, own):
        if a == 3:
            src = sb.at[plane + block]
            dst = sb.at[block]
        else:
            src = qkv_src(a, p) if own else kv_dst(a, plane + block)
            dst = kv_dst(a, block)
        return rdma(src, dst, s_halo.at[block, a], r_halo.at[block, a], (sp + plane, tp))

    def weight_dst(s, a):
        if a == 0:
            return ga.at[pl.ds(mul(s, depth), depth), :]
        if a == 1:
            return ua.at[pl.ds(mul(s, depth), depth), :]
        return da.at[:, pl.ds(mul(s, depth), depth)]

    def weight_src(line, a):
        at = pl.ds(mul(line, units), units)
        if a == 0:
            return gate.at[:, at]
        if a == 1:
            return up.at[:, at]
        return down.at[at, :]

    def w1_copy(d, a):
        zz = line_peer(d)
        return rdma(weight_src(zz, a), weight_dst(sp, a), s_w1.at[d - 1, a], r_w.at[sp, a], (zz * plane + p, tp))

    def w2_copy(k, d, a):
        s = line_peer(d) * plane + p
        src = weight_src(z, a) if d == 0 else weight_dst(s, a)
        return rdma(src, weight_dst(s, a), s_w2.at[k - 1, d, a], r_w.at[s, a], (z * plane + peer(k), tp))

    def relay_copy(d, a):
        k = 1 + (d + a) % 2
        s = line_peer(d) * plane + peer(k)
        return rdma(weight_dst(s, a), weight_dst(s, a), s_relay.at[d, a], r_w.at[s, a], (z * plane + peer(3 - k), tp))

    def weight_arrived(d, a, q):
        s = line_peer(d) * plane + q
        arrived(weight_dst(s, a), r_w.at[s, a])

    def spread(d, a):
        if d > 0:
            weight_arrived(d, a, p)
        for k in (1, 2):
            w2_copy(k, d, a).start()

    def relay(d, a):
        weight_arrived(d, a, peer(1 + (d + a) % 2))
        relay_copy(d, a).start()

    def rest_of_weights(a):
        for d in range(lines):
            weight_arrived(d, a, peer(2 - (d + a) % 2))
            weight_arrived(d, a, peer(3))

    def arrived(dst, sem):
        rdma(dst, dst, s_pair.at[0], sem, partner).wait_recv()

    def local(src, dst, i):
        return pltpu.make_async_copy(src, dst, s_loc.at[i])

    sb[plane + p] = seg[...].reshape(1, rows)
    for k in range(plane - 1):
        for a in (0, 1, 2, 5):
            qkv_copy(k, a).start()
    for k in range(plane - 1):
        for a in (3, 4):
            qkv_copy(k, a).start()

    @pl.when(z < lines - 1)
    def _():
        for a in range(4):
            halo_copy(p, a, True).start()

    for a in range(3):
        for d in range(1, lines):

            @pl.when(line_peer(d) < z)
            def _():
                w1_copy(d, a).start()

    locals_ = [local(qkv_src(a, p), qkv_dst(a, p), a) for a in range(5)]
    locals_.append(local(out_w, oww, 5))
    locals_.append(local(resid, res, 6))
    for a in range(3):
        locals_.append(local(weight_src(z, a), weight_dst(sp, a), 7 + a))
    for c in locals_:
        c.start()
    mg[tp] = mix_gain[...]
    rdma(mix_gain, mg.at[tp], s_pair.at[0], r_pair.at[0], partner).start()

    for a in range(2):
        spread(0, a)

    @pl.when(z == 0)
    def _():
        vb[: plane * rows, :] = jnp.zeros((plane * rows, VD), vb.dtype)
        kb[:, : plane * rows, :] = jnp.zeros((2, plane * rows, HD), kb.dtype)
        for b in range(plane):
            sb[b] = jnp.full(sb.shape[1:], -1, sb.dtype)

    nearest = jnp.maximum(peer(1), peer(2))
    other = jnp.minimum(peer(1), peer(2))
    for q in (nearest, jnp.maximum(other, peer(3)), jnp.minimum(other, peer(3))):
        for a in (0, 1, 2, 5):
            arrived(qkv_dst(a, q), r_qkv.at[q, a])

        @pl.when(z < lines - 1)
        def _():
            for a in range(4):
                halo_copy(q, a, False).start()

    for k in range(plane - 1):
        q = in_plane[k]
        for a in (3, 4):
            arrived(qkv_dst(a, q), r_qkv.at[q, a])
    for c in locals_[:5]:
        c.wait()

    scale = HD ** (-0.5) * 1.4426950408889634
    window = (REACH + 1) * rows

    def ao_remote(j):
        at = pl.ds(mul(tp * heads + p, VD), VD)
        return rdma(ao.at[j], ar.at[:, at], s_ao.at[j], r_ao.at[p], (z * plane + j, tp))

    def ao_local(j):
        at = pl.ds(mul(tp * heads + p, VD), VD)
        return local(ao.at[j], ar.at[:, at], 10)

    coef = lam[p]

    def query_block(i, carry):
        j = plane - 1 - i

        @pl.when(z > 0)
        def _():
            for a in range(3):
                arrived(kv_dst(a, j), r_halo.at[j, a])
            arrived(sb.at[j], r_halo.at[j, 3])

        for a in range(3):
            for d in range(1, lines):

                @pl.when((i == plane - 1) & (line_peer(d) > z))
                def _():
                    w1_copy(d, a).start()

        at = pl.ds(mul(j, rows), window)
        key_seg = jnp.concatenate([sb[j + n] for n in range(REACH + 1)], axis=1).astype(jnp.float32)
        own_seg = jnp.broadcast_to(sb[plane + j].astype(jnp.float32), (128, rows))
        seg_col = jnp.transpose(own_seg)[:, :1]
        for u in range(rows // sub):
            col = lax.broadcasted_iota(jnp.int32, (sub, window), 1)
            row = lax.broadcasted_iota(jnp.int32, (sub, window), 0) + (REACH * rows + u * sub)
            ok = (key_seg == seg_col[u * sub : (u + 1) * sub]) & (col <= row)
            outs = []
            for m in range(2):
                q = qb[m, pl.ds(pl.multiple_of(j * rows + u * sub, sub), sub), :]
                s = lax.dot_general(
                    q, kb[m, at, :], (((1,), (1,)), ((), ())), preferred_element_type=jnp.float32
                )
                s = jnp.where(ok, s, -1e30)
                top = jnp.max(s, axis=1, keepdims=True)
                e = jnp.exp2((s - top) * scale)
                total = jnp.sum(e, axis=1, keepdims=True)
                o = jnp.dot(e.astype(jnp.bfloat16), vb[at, :], preferred_element_type=jnp.float32)
                outs.append(o / total)
            h = outs[0] - coef * outs[1]
            ms = jnp.mean(h * h, axis=1, keepdims=True)
            h = h * lax.rsqrt(ms + 1e-05) * head_gain[...]
            ao[j, pl.ds(u * sub, sub), :] = h.astype(ao.dtype)

        @pl.when(j != p)
        def _():
            ao_remote(j).start()

        @pl.when(j == p)
        def _():
            ao_local(j).start()

        return carry

    lax.fori_loop(0, plane, query_block, 0)
    spread(0, 2)
    relay(0, 0)
    relay(0, 1)

    ao_local(p).wait()
    for q in in_plane:
        at = pl.ds(mul(tp * heads + q, VD), VD)
        arrived(ar.at[:, at], r_ao.at[q])
    mine = pl.ds(mul(tp, half), half)
    theirs = pl.ds(mul(1 - tp, half), half)
    swap = rdma(ar.at[:, mine], ar.at[:, mine], s_pair.at[1], r_pair.at[1], partner)
    swap.start()
    for c in locals_[5:7]:
        c.wait()
    acc = jnp.dot(ar[:, mine], oww[mine, :], preferred_element_type=jnp.float32)
    arrived(ar.at[:, theirs], r_pair.at[1])
    acc = acc + jnp.dot(ar[:, theirs], oww[theirs, :], preferred_element_type=jnp.float32)
    mid[tp] = (res[...].astype(jnp.float32) + acc).astype(mid.dtype)
    swap_mid = rdma(mid.at[tp], mid.at[tp], s_pair.at[2], r_pair.at[2], partner)
    swap_mid.start()
    arrived(mid.at[1 - tp], r_pair.at[2])
    arrived(mg.at[1 - tp], r_pair.at[0])
    m0, m1 = mid[0].astype(jnp.float32), mid[1].astype(jnp.float32)
    squares = jnp.sum(m0 * m0, axis=1, keepdims=True) + jnp.sum(m1 * m1, axis=1, keepdims=True)
    inv = lax.rsqrt(squares / (2 * half) + 1e-06)
    xa[z, 0] = (m0 * inv * mg[0]).astype(xa.dtype)
    xa[z, 1] = (m1 * inv * mg[1]).astype(xa.dtype)

    piece = rows // pieces

    def ag_copy(b, to, c):
        ref = xa.at[b, tp, pl.ds(c * piece, piece), :]
        return rdma(ref, ref, s_ag.at[b, to, c], r_ag.at[b, c], (sp + plane * (2 * to - 1), tp))

    def xd_copy(b):
        return rdma(xa.at[b, tp], xa.at[b, tp], s_xd.at[b], r_xd.at[b], partner)

    for c in range(pieces):

        @pl.when(z < lines - 1)
        def _():
            ag_copy(z, 1, c).start()

        @pl.when(z > 0)
        def _():
            ag_copy(z, 0, c).start()

    def from_above(d):
        above = z + d

        @pl.when(above < lines)
        def _():
            for c in range(pieces):
                arrived(xa.at[above, tp, pl.ds(c * piece, piece), :], r_ag.at[above, c])

                @pl.when(z > 0)
                def _():
                    ag_copy(above, 0, c).start()

            xd_copy(above).start()

    def from_below(d):
        below = z - d

        @pl.when(below >= 0)
        def _():
            for c in range(pieces):
                arrived(xa.at[below, tp, pl.ds(c * piece, piece), :], r_ag.at[below, c])

                @pl.when(z < lines - 1)
                def _():
                    ag_copy(below, 1, c).start()

            xd_copy(below).start()

    tile = units // 3

    def hidden_block(b):
        @pl.when(b != z)
        def _():
            arrived(xa.at[b, 1 - tp], r_xd.at[b])

        def hidden_tile(u, carry):
            at = pl.ds(mul(u, tile), tile)
            g = jnp.dot(xa[b, 0], ga[:half, at], preferred_element_type=jnp.float32)
            g = g + jnp.dot(xa[b, 1], ga[half:, at], preferred_element_type=jnp.float32)
            v = jnp.dot(xa[b, 0], ua[:half, at], preferred_element_type=jnp.float32)
            v = v + jnp.dot(xa[b, 1], ua[half:, at], preferred_element_type=jnp.float32)
            hid[b, :, at] = (g / (1.0 + jnp.exp(-g)) * v).astype(hid.dtype)
            return carry

        lax.fori_loop(0, units // tile, hidden_tile, 0)

    def next_block(i):
        upper = lines - 1 - z
        return jnp.where(i < upper, z + 1 + i, z - 1 - (i - upper))

    for d in range(1, lines):
        spread(d, 0)
    relay(0, 2)
    for d in range(1, lines):
        spread(d, 1)
    for d in range(1, lines):
        relay(d, 0)
    from_above(1)
    for d in range(1, lines):
        relay(d, 1)
        spread(d, 2)
    inner = (z > 1) & (z < lines - 1)
    from_above(2)

    @pl.when(jnp.logical_not(inner))
    def _():
        from_below(1)

    def rank(zz):
        first = list(range(lines - 1, 0, -1))
        last = list(range(lines - 2, -1, -1))
        travel = [
            (first.index(b) + zz if b > zz else last.index(b) + lines - 1 - zz, -b) for b in range(lines) if b != zz
        ]
        return [-b for _, b in sorted(travel)] + [zz]

    def order(i):
        b = rank(0)[i]
        for zz in range(1, lines):
            b = jnp.where(z == zz, rank(zz)[i], b)
        return b

    relay(1, 2)

    @pl.when(inner)
    def _():
        from_below(1)

    for c in locals_[7:]:
        c.wait()
    rest_of_weights(0)
    rest_of_weights(1)

    @pl.when(z == lines - 1)
    def _():
        hidden_block(order(0))

    @pl.when(z < lines - 1)
    def _():
        hidden_block(z)

    for d in range(2, lines):
        relay(d, 2)

    @pl.when(inner)
    def _():
        from_below(2)

    at_end = (z == 0) | (z == lines - 1)
    wide = half // 2

    def down_block(b):
        def down_tile(c, carry):
            theirs_at = pl.ds(pl.multiple_of((1 - tp) * half + c * wide, wide), wide)
            own_at = pl.ds(pl.multiple_of(tp * half + c * wide, wide), wide)
            at = pl.ds(mul(c, wide), wide)
            o = jnp.dot(hid[b], da[:, theirs_at], preferred_element_type=jnp.float32)
            psend[b, :, at] = o.astype(psend.dtype)
            o = jnp.dot(hid[b], da[:, own_at], preferred_element_type=jnp.float32)
            pown[b, :, at] = o
            return carry

        lax.fori_loop(0, half // wide, down_tile, 0)
        rdma(psend.at[b], precv.at[b], s_pp.at[b], r_pp.at[b], partner).start()

    def chain_copy(b, to, c):
        near = jnp.where(b == z + 1, lines, b) if to == 1 else b
        at = pl.ds(c * piece, piece)
        return rdma(
            csend.at[b, at, :], crecv.at[near, at, :], s_ch.at[b, c], r_ch.at[near, c],
            (sp + plane * (2 * to - 1), tp),
        )

    def chain(b, lo=0, hi=pieces):
        if lo == 0:
            arrived(precv.at[b], r_pp.at[b])
        incoming = ((b < z) & (z < lines - 1)) | ((b > z) & (z > 0))
        for c in range(lo, hi):
            at = pl.ds(c * piece, piece)

            @pl.when(incoming)
            def _():
                arrived(crecv.at[b, at, :], r_ch.at[b, c])
                own = pown[b, at, :] + precv[b, at, :].astype(jnp.float32)
                csend[b, at, :] = (own + crecv[b, at, :].astype(jnp.float32)).astype(csend.dtype)

            @pl.when(jnp.logical_not(incoming))
            def _():
                own = pown[b, at, :] + precv[b, at, :].astype(jnp.float32)
                csend[b, at, :] = own.astype(csend.dtype)

            @pl.when(b > z)
            def _():
                chain_copy(b, 1, c).start()

            @pl.when(b < z)
            def _():
                chain_copy(b, 0, c).start()

    @pl.when(at_end)
    def _():
        for i in range(3, lines):
            from_above(i)
        for i in range(lines - 1):
            if i > 0:
                from_below(i + 1)
            if i == 0:

                @pl.when(z == 0)
                def _():
                    hidden_block(order(0))

                rest_of_weights(2)
            if i > 0:
                hidden_block(order(i))
            down_block(order(i))
            if i == 0:
                chain(order(i), 0, pieces // 2)

                @pl.when(z == 0)
                def _():
                    chain(order(i), pieces // 2)

            else:
                chain(order(i))

        @pl.when(z > 0)
        def _():
            chain(order(0), pieces // 2)
            hidden_block(z)

        down_block(z)


    @pl.when(jnp.logical_not(at_end))
    def _():
        @pl.when(jnp.logical_not(inner))
        def _():
            from_below(2)

        for i in range(3, lines):
            from_above(i)
            from_below(i)
        for i in range(lines - 1):
            hidden_block(next_block(i))
        rest_of_weights(2)
        for i in range(lines):
            down_block(order(i))
        for i in range(lines - 1):
            chain(order(i))

    arrived(precv.at[z], r_pp.at[z])
    pown[z] = pown[z] + precv[z].astype(jnp.float32) + mid[tp].astype(jnp.float32)
    for c in range(pieces):
        at = pl.ds(c * piece, piece)

        @pl.when(z < lines - 1)
        def _():
            arrived(crecv.at[z, at, :], r_ch.at[z, c])
            pown[z, at, :] = pown[z, at, :] + crecv[z, at, :].astype(jnp.float32)

        @pl.when(z > 0)
        def _():
            arrived(crecv.at[lines, at, :], r_ch.at[lines, c])
            pown[z, at, :] = pown[z, at, :] + crecv[lines, at, :].astype(jnp.float32)

        out[at, :] = pown[z, at, :].astype(out.dtype)

    for k in range(plane - 1):
        for a in range(6):
            qkv_copy(k, a).wait_send()
    for d in range(lines):
        for a in range(3):
            w2_copy(1, d, a).wait_send()
            w2_copy(2, d, a).wait_send()
            relay_copy(d, a).wait_send()
    for d in range(1, lines):
        for a in range(3):
            w1_copy(d, a).wait_send()

    @pl.when(z < lines - 1)
    def _():
        for a in range(4):
            halo_copy(p, a, True).wait_send()
            for q in in_plane:
                halo_copy(q, a, False).wait_send()

    for q in in_plane:
        ao_remote(q).wait_send()
    rdma(mix_gain, mg.at[tp], s_pair.at[0], r_pair.at[0], partner).wait_send()
    swap.wait_send()
    swap_mid.wait_send()
    for b in range(lines):
        rdma(psend.at[b], precv.at[b], s_pp.at[b], r_pp.at[b], partner).wait_send()

        @pl.when(b != z)
        def _():
            xd_copy(b).wait_send()

        @pl.when((b <= z) & (z < lines - 1))
        def _():
            for c in range(pieces):
                ag_copy(b, 1, c).wait_send()

        @pl.when((b >= z) & (z > 0))
        def _():
            for c in range(pieces):
                ag_copy(b, 0, c).wait_send()

        @pl.when(b > z)
        def _():
            for c in range(pieces):
                chain_copy(b, 1, c).wait_send()

        @pl.when(b < z)
        def _():
            for c in range(pieces):
                chain_copy(b, 0, c).wait_send()


def fast_body(resid, query_one, key_one, query_two, key_two, values, mix_lambda, segments, head_gain,
              out_weight, mixer_gain, gate_weight, up_weight, down_weight):
    plane = mix_lambda.shape[0]
    lines = lax.axis_size("sp") // plane
    rows, half = resid.shape
    depth, units = gate_weight.shape[0], gate_weight.shape[1] // lines
    full = depth * plane * lines
    bf, f32 = jnp.bfloat16, jnp.float32
    sub = rows // 3
    pieces = 8
    dma = pltpu.SemaphoreType.DMA
    anywhere = pl.BlockSpec(memory_space=pl.ANY)
    vmem = pl.BlockSpec(memory_space=pltpu.VMEM)
    smem = pl.BlockSpec(memory_space=pltpu.SMEM)
    flops = 6 * rows * plane * full * units + 2 * rows * full * half + 24 * rows * plane * rows * 5 * VD
    return pl.pallas_call(
        functools.partial(layer_kernel, plane, lines, sub, pieces),
        out_shape=jax.ShapeDtypeStruct((rows, half), bf),
        in_specs=[anywhere] * 6 + [smem, vmem, vmem, anywhere, vmem, anywhere, anywhere, anywhere],
        out_specs=vmem,
        scratch_shapes=[
            pltpu.VMEM((2, plane * rows, HD), bf),
            pltpu.VMEM((2, 2 * plane * rows, HD), bf),
            pltpu.VMEM((2 * plane * rows, VD), bf),
            pltpu.VMEM((2 * plane, 1, rows), jnp.int32),
            pltpu.VMEM((plane, rows, VD), bf),
            pltpu.VMEM((rows, full), bf),
            pltpu.VMEM((full, half), bf),
            pltpu.VMEM((rows, half), bf),
            pltpu.VMEM((2, rows, half), bf),
            pltpu.VMEM((2, 1, half), f32),
            pltpu.VMEM((lines, 2, rows, half), bf),
            pltpu.VMEM((full, units), bf),
            pltpu.VMEM((full, units), bf),
            pltpu.VMEM((units, full), bf),
            pltpu.VMEM((lines, rows, units), bf),
            pltpu.VMEM((lines, rows, half), f32),
            pltpu.VMEM((lines, rows, half), bf),
            pltpu.VMEM((lines, rows, half), bf),
            pltpu.VMEM((lines, rows, half), bf),
            pltpu.VMEM((lines + 1, rows, half), bf),
            dma((plane - 1, 6)), dma((plane, 6)),
            dma((plane, 4)), dma((plane, 4)),
            dma((lines - 1, 3)), dma((2, lines, 3)), dma((lines, 3)), dma((plane * lines, 3)),
            dma((plane,)), dma((plane,)),
            dma((3,)), dma((3,)),
            dma((lines, 2, pieces)), dma((lines, pieces)),
            dma((lines,)), dma((lines,)),
            dma((lines,)), dma((lines,)),
            dma((lines, pieces)), dma((lines + 1, pieces)),
            dma((11,)),
        ],
        compiler_params=pltpu.CompilerParams(
            collective_id=0, has_side_effects=True, vmem_limit_bytes=60 * 1024 * 1024
        ),
        cost_estimate=pl.CostEstimate(flops=flops, bytes_accessed=2 * full * units, transcendentals=0),
        name="layer",
    )(resid, query_one, key_one, query_two, key_two, values, mix_lambda, segments,
      head_gain.reshape(1, VD), out_weight, mixer_gain.reshape(1, half), gate_weight, up_weight, down_weight)


def fits(mesh):
    sp, tp = mesh.shape["sp"], mesh.shape["tp"]
    return tp == 2 and sp % (REACH * 2) == 0


def choose(mesh):
    def step(*args):
        heads = args[6].shape[0]
        if fits(mesh) and heads == REACH:
            return fast_body(*args)
        return body(*args)

    return step


def solution(mesh):
    in_specs = (
        P("sp", "tp"),
        P("sp", "tp"),
        P("sp", "tp"),
        P("sp", "tp"),
        P("sp", "tp"),
        P("sp", "tp"),
        P("tp"),
        P("sp"),
        P(),
        P(None, "tp"),
        P("tp"),
        P("sp", "tp"),
        P("sp", "tp"),
        P("tp", "sp"),
    )
    out_specs = P("sp", "tp")
    return jax.shard_map(choose(mesh), mesh=mesh, in_specs=in_specs, out_specs=out_specs, check_vma=False)
```
